1024 devices in a mesh: sp: 128 (over z, y), tp: 8 (over x, core).
Axes of the slice: x: 4, y: 8, z: 16, core: 2. Of those that a mesh axis runs over, the one named last changes fastest.
Arguments:
- latent: bfloat16 [32768, 2048], P('sp'), may hold values from -6 to 6
- context: bfloat16 [512, 2048], P('sp'), may hold values from -6 to 6
- condition: float32 [2048], P('sp'), may hold values from -6 to 6
- ctx_condition: float32 [2048], P('sp'), may hold values from -6 to 6
- shift_weight: bfloat16 [2048, 2048], P('sp', 'tp'), may hold values from -0.125 to 0.125
- scale_weight: bfloat16 [2048, 2048], P('sp', 'tp'), may hold values from -0.125 to 0.125
- gate_weight: bfloat16 [2048, 2048], P('sp', 'tp'), may hold values from -0.125 to 0.125
- norm_gain: float32 [2048], replicated, may hold values from 0.1 to 1.9
- query_weight: bfloat16 [2048, 1024], P(None, 'tp'), may hold values from -0.125 to 0.125
- key_weight: bfloat16 [2048, 1024], P(None, 'tp'), may hold values from -0.125 to 0.125
- value_weight: bfloat16 [2048, 1024], P(None, 'tp'), may hold values from -0.125 to 0.125
- query_gain: float32 [64], replicated, may hold values from 0.6 to 6.5
- key_gain: float32 [64], replicated, may hold values from 0.6 to 6.5
- offset_bias: float32 [16, 15, 31], P('tp'), may hold values from 1 to 3
- out_weight: bfloat16 [1024, 2048], P('tp'), may hold values from -0.75 to 0.75
Outputs:
- mixed_rows: bfloat16 [32768, 2048], P('sp')
The draws below stay inside these ranges and needn't reach their ends.
All inputs are finite; a program needn't handle non-finite values.
Results may differ from the reference program's by a relative error of at most 0.01405.
The reference program's roundings to bfloat16 on the way count: a program that leaves them out, or rounds other values in their place, can miss the bound.
Values may be sent and summed in bfloat16 or wider, within the bound.
A program may use at most 64 MiB of HBM per device.

```python
import jax
import jax.numpy as jnp
from jax import lax

D = 2048
HEADS = 16
HEAD_DIM = 64
GRID_W = 64
WIN_ROWS = 8
WIN_COLS = 16
CTX = 512
TOKENS = 32768
ATT_W = 1024
N_TP = 8


def gain_draw(base_key):
    return jax.random.uniform(base_key, (HEAD_DIM,), jnp.float32, 0.6, 2.0)


def draw_query_gain(key, part):
    return gain_draw(jax.random.fold_in(key, 11))


def draw_key_gain(key, part):
    return gain_draw(jax.random.fold_in(key, 23))


def level_of(stream_key, dims, cuts, smallest, largest):
    gain = 1.0
    for dim, shards_of in cuts:
        heights = jax.random.uniform(jax.random.fold_in(jax.random.fold_in(stream_key, 6), dim), (shards_of,), jnp.float32, smallest / len(cuts), largest / len(cuts))
        gain = gain * jnp.repeat(jnp.exp(heights), dims[dim] // shards_of).reshape((-1,) + (1,) * (len(dims) - 1 - dim))
    return gain


def gaussian(rng, extent, width, most, cuts=(), kind=jnp.bfloat16):
    values = width * jax.random.normal(rng, extent, jnp.float32)
    if cuts:
        values = values * level_of(rng, extent, cuts, -0.22, 0.18)
    return jnp.clip(values, -most, most).astype(kind)


def setup_inputs(seed: int = 0) -> dict:
    streams_of = jax.random.split(jax.random.key(seed), 16)
    latent = gaussian(streams_of[0], (TOKENS, D), 1.0, 6.0, ((0, 128),))
    context = gaussian(streams_of[1], (CTX, D), 1.0, 6.0, ((0, 128),))
    condition = gaussian(streams_of[2], (D,), 1.0, 6.0, ((0, 128),), jnp.float32)
    ctx_condition = gaussian(streams_of[3], (D,), 1.0, 6.0, ((0, 128),), jnp.float32)
    shift_weight = gaussian(streams_of[4], (D, D), D ** -0.5, 0.125, ((0, 128), (1, 8)))
    scale_weight = gaussian(streams_of[5], (D, D), D ** -0.5, 0.125, ((0, 128), (1, 8)))
    gate_weight = gaussian(streams_of[6], (D, D), D ** -0.5, 0.125, ((0, 128), (1, 8)))
    norm_gain = jnp.clip(1.0 + 0.18 * jax.random.normal(streams_of[7], (D,), jnp.float32), 0.1, 1.9)
    query_weight = gaussian(streams_of[8], (D, ATT_W), D ** -0.5, 0.125, ((1, 8),))
    key_weight = gaussian(streams_of[9], (D, ATT_W), D ** -0.5, 0.125, ((1, 8),))
    value_weight = gaussian(streams_of[10], (D, ATT_W), D ** -0.5, 0.125, ((1, 8),))
    query_gain = draw_query_gain(jax.random.fold_in(streams_of[15], 71), 0)
    key_gain = draw_key_gain(jax.random.fold_in(streams_of[15], 71), 0)
    offset_bias = jnp.clip(1.0 + 2.0 * jax.random.uniform(streams_of[13], (HEADS, 2 * WIN_ROWS - 1, 2 * WIN_COLS - 1), jnp.float32) ** level_of(streams_of[13], (HEADS, 2 * WIN_ROWS - 1, 2 * WIN_COLS - 1), ((0, 8),), -0.2, 0.2), 1.0, 3.0)
    out_weight = gaussian(streams_of[14], (ATT_W, D), (ATT_W // 16) ** -0.5, 0.75, ((0, 8),))
    return dict(latent=latent, context=context, condition=condition, ctx_condition=ctx_condition, shift_weight=shift_weight, scale_weight=scale_weight, gate_weight=gate_weight, norm_gain=norm_gain, query_weight=query_weight, key_weight=key_weight, value_weight=value_weight, query_gain=query_gain, key_gain=key_gain, offset_bias=offset_bias, out_weight=out_weight)


EPS = 1e-06

def modulate(rows_in, norm_gain, shift_vec, scale_vec):
    values = rows_in.astype(jnp.float32)
    normed = values * lax.rsqrt(lax.optimization_barrier(jnp.mean(values * values, axis=-1, keepdims=True)) + EPS)
    return (normed * norm_gain * (1.0 + scale_vec) + shift_vec).astype(jnp.bfloat16)

def head_norm(projected, head_gain):
    row_count = projected.shape[0]
    split_heads = projected.reshape(row_count, -1, head_gain.shape[0])
    normed = split_heads * lax.rsqrt(lax.optimization_barrier(jnp.mean(split_heads * split_heads, axis=-1, keepdims=True)) + EPS)
    return (normed * head_gain).astype(jnp.bfloat16).reshape(row_count, -1)

def per_head(matrix, row_count):
    return matrix.reshape(row_count, HEADS, HEAD_DIM).transpose(1, 0, 2)

def reference(latent, context, condition, ctx_condition, shift_weight, scale_weight, gate_weight, norm_gain, query_weight, key_weight, value_weight, query_gain, key_gain, offset_bias, out_weight):
    activations = jax.nn.silu(jnp.stack([condition, ctx_condition])).astype(jnp.bfloat16)
    shift_vec = jnp.dot(activations, shift_weight, preferred_element_type=jnp.float32)
    scale_vec = jnp.dot(activations, scale_weight, preferred_element_type=jnp.float32)
    gate_vec = jnp.dot(activations[:1], gate_weight, preferred_element_type=jnp.float32)
    hidden = modulate(latent, norm_gain, shift_vec[0], scale_vec[0])
    ctx_hidden = modulate(context, norm_gain, shift_vec[1], scale_vec[1])
    queries = head_norm(jnp.dot(hidden, query_weight, preferred_element_type=jnp.float32), query_gain)
    keys_lat = head_norm(jnp.dot(hidden, key_weight, preferred_element_type=jnp.float32), key_gain)
    values_lat = jnp.dot(hidden, value_weight, preferred_element_type=jnp.float32).astype(jnp.bfloat16)
    ctx_keys = head_norm(jnp.dot(ctx_hidden, key_weight, preferred_element_type=jnp.float32), key_gain)
    ctx_values = jnp.dot(ctx_hidden, value_weight, preferred_element_type=jnp.float32).astype(jnp.bfloat16)
    grid_rows = TOKENS // GRID_W
    score_scale = HEAD_DIM ** (-0.5)
    row_ids = jnp.arange(grid_rows, dtype=jnp.int32)
    band_start = jnp.clip(row_ids - WIN_ROWS // 2, 0, grid_rows - WIN_ROWS)
    band_rows = band_start[:, None] + jnp.arange(WIN_ROWS, dtype=jnp.int32)[None, :]
    row_steps = band_rows - row_ids[:, None] + WIN_ROWS - 1
    column_ids = jnp.arange(GRID_W, dtype=jnp.int32)
    col_start = jnp.clip(column_ids - WIN_COLS // 2, 0, GRID_W - WIN_COLS)
    col_open = (column_ids[None, :] >= col_start[:, None]) & (column_ids[None, :] < col_start[:, None] + WIN_COLS)
    col_steps = jnp.clip(column_ids[None, :] - column_ids[:, None], 1 - WIN_COLS, WIN_COLS - 1) + WIN_COLS - 1

    def one_head(operands):
        q_head, k_head, v_head, kc_head, vc_head, table = operands
        q_grid = q_head.reshape(grid_rows, GRID_W, HEAD_DIM).astype(jnp.float32)
        k_grid = k_head.reshape(grid_rows, GRID_W, HEAD_DIM).astype(jnp.float32)
        v_grid = v_head.reshape(grid_rows, GRID_W, HEAD_DIM).astype(jnp.float32)
        k_band = k_grid[band_rows]
        v_band = v_grid[band_rows]
        offsets = table[row_steps[:, None, :, None], col_steps[None, :, None, :]]
        local_scores = jnp.einsum('rqd,rjkd->rqjk', q_grid, k_band) * score_scale + offsets
        local_scores = jnp.where(col_open[None, :, None, :], local_scores, -jnp.inf)
        ctx_scores = jnp.einsum('rqd,nd->rqn', q_grid, kc_head.astype(jnp.float32)) * score_scale
        row_max = jnp.maximum(lax.optimization_barrier(jnp.max(local_scores, axis=(2, 3))), lax.optimization_barrier(jnp.max(ctx_scores, axis=2)))
        local_exp = jnp.exp(local_scores - row_max[..., None, None])
        ctx_exp = jnp.exp(ctx_scores - row_max[..., None])
        denominator = lax.optimization_barrier(jnp.sum(local_exp, axis=(2, 3))) + lax.optimization_barrier(jnp.sum(ctx_exp, axis=2))
        local_weights = (local_exp / denominator[..., None, None]).astype(jnp.bfloat16)
        ctx_weights = (ctx_exp / denominator[..., None]).astype(jnp.bfloat16)
        result = jnp.einsum('rqjk,rjkd->rqd', local_weights.astype(jnp.float32), v_band) + jnp.einsum('rqn,nd->rqd', ctx_weights.astype(jnp.float32), vc_head.astype(jnp.float32))
        return result.astype(jnp.bfloat16)
    attended = lax.map(one_head, (per_head(queries, TOKENS), per_head(keys_lat, TOKENS), per_head(values_lat, TOKENS), per_head(ctx_keys, CTX), per_head(ctx_values, CTX), offset_bias))
    attended = attended.transpose(1, 2, 0, 3).reshape(TOKENS, ATT_W)
    group_cols = ATT_W // N_TP
    branch = jnp.zeros((TOKENS, D), jnp.float32)
    for group in range(N_TP):
        partial_value = jnp.dot(attended[:, group * group_cols:(group + 1) * group_cols], out_weight[group * group_cols:(group + 1) * group_cols], preferred_element_type=jnp.float32)
        rounded = lax.optimization_barrier(partial_value.astype(jnp.bfloat16))
        branch = branch + rounded.astype(jnp.float32)
    return (latent.astype(jnp.float32) + gate_vec[0] * branch).astype(jnp.bfloat16)
```

```python
import jax
import jax.numpy as jnp
from jax import lax
from jax.experimental import pallas as pl
from jax.experimental.pallas import tpu as pltpu
from jax.sharding import PartitionSpec as P

MESH = pl.DeviceIdType.MESH
EPS = 1e-06
Z, Y, TP = 16, 8, 8
SP = Z * Y
D = 2048
F = D // TP
TOK = 256
COLS = 64
ROWS = 4
HD = 64
NEG = float("-inf")


def rem(a, n):
    return lax.rem(a, jnp.int32(n))


def head_norm(p, gain2):
    lane = lax.broadcasted_iota(jnp.int32, p.shape, 1)
    left = lane < HD
    sq = p * p
    s0 = jnp.sum(jnp.where(left, sq, 0.0), axis=1, keepdims=True)
    s1 = jnp.sum(jnp.where(left, 0.0, sq), axis=1, keepdims=True)
    r0 = lax.rsqrt(s0 * (1.0 / HD) + EPS)
    r1 = lax.rsqrt(s1 * (1.0 / HD) + EPS)
    return p * jnp.where(left, r0, r1) * gain2


def kernel(
    latent, context, cond, cctx, shw, scw, gw, gain, wq, wk, wv, qg, kg, bias, outw,
    out,
    part, mody, zpart, modz, modf,
    cbuf, cf, ckv,
    hbuf, xn, hid,
    wqv, wkvv, wfull, latv,
    tbl, kpad, vpad, q2, ew, attb, outv,
    loc_sem, out_sem,
    ys, yr, zs, zr, ts, tr,
    czs, czr, cts, ctr, cys, cyr,
    hs, hr, hps, hpr,
    ws, wr, wps, wpr,
    as_, ar,
):
    sp = lax.axis_index("sp")
    tp = lax.axis_index("tp")
    y = rem(sp, Y)
    z = lax.div(sp, jnp.int32(Y))
    c = rem(tp, 2)
    partner = tp + 1 - 2 * c
    up = rem(sp + 1, SP)
    down = rem(sp + SP - 1, SP)
    right = rem(tp + 2, TP)
    left = rem(tp + TP - 2, TP)
    far = rem(tp + 4, TP)

    def y_peer(k):
        return {"sp": z * Y + rem(y + k, Y), "tp": tp}

    def z_peer(k):
        return {"sp": rem(z + k, Z) * Y + y, "tp": tp}

    def t_peer(k):
        return {"sp": sp, "tp": rem(tp + k, TP)}

    def at(s, t):
        return {"sp": s, "tp": t}

    def remote(src, dst, s, r, dev):
        return pltpu.make_async_remote_copy(
            src_ref=src, dst_ref=dst, send_sem=s, recv_sem=r, device_id=dev, device_id_type=MESH
        )

    sends = []

    def send(src, dst, s, r, dev):
        d = remote(src, dst, s, r, dev)
        d.start()
        sends.append(d)
        return d

    barrier = pltpu.get_barrier_semaphore()
    peers = [z_peer(k) for k in (8, 7, 9, 6, 10, 5, 11, 4, 12, 3, 13, 2, 14, 1, 15)]
    peers += [y_peer(k) for k in range(1, Y)]
    peers += [t_peer(k) for k in range(1, TP)]
    peers += [at(up, tp), at(down, tp)]
    for p in peers:
        pl.semaphore_signal(barrier, inc=1, device_id=p, device_id_type=MESH)

    ctx_col = pl.multiple_of(tp * F, F)
    own_c = pltpu.make_async_copy(context.at[:, pl.ds(ctx_col, F)], cbuf.at[tp, z], loc_sem.at[0])
    own_l = pltpu.make_async_copy(latent, latv, loc_sem.at[1])
    own_q = pltpu.make_async_copy(wq, wqv, loc_sem.at[2])
    own_k = pltpu.make_async_copy(wk, wkvv.at[:, pl.ds(0, 128)], loc_sem.at[3])
    own_v = pltpu.make_async_copy(wv, wkvv.at[:, pl.ds(128, 128)], loc_sem.at[4])
    own_w = pltpu.make_async_copy(outw, wfull.at[tp], loc_sem.at[5])
    own_c.start()
    own_l.start()
    own_w.start()
    own_q.start()
    own_k.start()
    own_v.start()

    row8 = lax.broadcasted_iota(jnp.int32, (8, 16), 0)
    pre = jnp.where(row8 == 0, jnp.broadcast_to(cond[...], (8, 16)), jnp.broadcast_to(cctx[...], (8, 16)))
    act = (pre / (1.0 + jnp.exp(-pre))).astype(jnp.bfloat16)
    p_sh = jnp.dot(act, shw[...], preferred_element_type=jnp.float32)
    p_sc = jnp.dot(act, scw[...], preferred_element_type=jnp.float32)
    p_g = jnp.dot(act, gw[...], preferred_element_type=jnp.float32)
    part[0:2, :] = p_sh[0:2]
    part[2:4, :] = p_sc[0:2]
    part[4:5, :] = p_g[0:1]

    pl.semaphore_wait(barrier, len(peers))

    for k in (4, 3, 5, 2, 6, 1, 7):
        send(part, mody.at[k - 1], ys.at[k - 1], yr.at[k - 1], y_peer(k))
    own_c.wait()
    for k in (8, 7, 9, 6, 10, 5, 11, 4, 12, 3, 13, 2, 14, 1, 15):
        send(cbuf.at[tp, z], cbuf.at[tp, z], czs.at[k - 1], czr.at[k - 1], z_peer(k))
    own_l.wait()
    own_w.wait()
    half = pl.ds(pl.multiple_of(c * 128, 128), 128)
    halo_up = send(latv.at[half], hbuf.at[0, half], hs.at[0], hr.at[0], at(up, tp))
    halo_dn = send(latv.at[half], hbuf.at[1, half], hs.at[1], hr.at[1], at(down, tp))
    w_right = send(wfull.at[tp], wfull.at[tp], ws.at[0], wr.at[0], at(sp, right))
    w_left = send(wfull.at[tp], wfull.at[tp], ws.at[1], wr.at[1], at(sp, left))
    send(wfull.at[tp], wfull.at[tp], wps.at[0], wpr.at[0], at(sp, partner))

    tq = lax.broadcasted_iota(jnp.int32, (COLS, 128), 0)
    tl = lax.broadcasted_iota(jnp.int32, (COLS, 128), 1)
    tk = jnp.where(tl < COLS, tl, tl - COLS)
    diff = tk - tq + 15
    c0 = jnp.clip(tq - 8, 0, 48)
    is_open = (tk >= c0) & (tk < c0 + 16)
    first = lax.broadcasted_iota(jnp.int32, (1, 128), 1) < COLS

    def table_step(n, carry):
        h = lax.div(n, jnp.int32(14))
        a = rem(n, 14)
        val = jnp.full((COLS, 128), NEG, jnp.float32)
        for dd in range(31):
            v = jnp.where(first, bias[h, a, dd], bias[h, a + 1, dd])
            val = jnp.where(diff == dd, jnp.broadcast_to(v, (COLS, 128)), val)
        tbl[h, a] = jnp.where(is_open, val, NEG)
        return carry

    lax.fori_loop(0, 28, table_step, 0)

    def normed(load, store, rows, chunk):
        def step(n, carry):
            r = pl.ds(pl.multiple_of(n * chunk, chunk), chunk)
            v = load(r).astype(jnp.float32)
            ms = jnp.mean(v * v, axis=-1, keepdims=True)
            store(r, v * lax.rsqrt(ms + EPS) * gain[...])
            return carry

        lax.fori_loop(0, rows // chunk, step, 0)

    acc = part[...]
    for k in range(1, Y):
        remote(part, mody.at[k - 1], ys.at[k - 1], yr.at[k - 1], y_peer(k)).wait_recv()
        acc = acc + mody[k - 1]
    zpart[...] = acc
    for k in (8, 7, 9, 6, 10, 5, 11, 4, 12, 3, 13, 2, 14, 1, 15):
        send(zpart, modz.at[k - 1], zs.at[k - 1], zr.at[k - 1], z_peer(k))

    def store_own(r, v):
        xn[1, r, :] = v

    normed(lambda r: latv[r, :], store_own, TOK, 16)

    for k in range(1, Z):
        remote(cbuf.at[tp, z], cbuf.at[tp, z], czs.at[k - 1], czr.at[k - 1], z_peer(k)).wait_recv()
    for k in range(1, TP):
        send(cbuf.at[tp], cbuf.at[tp], cts.at[k - 1], ctr.at[k - 1], t_peer(k))

    acc = zpart[...]
    for k in range(1, Z):
        remote(zpart, modz.at[k - 1], zs.at[k - 1], zr.at[k - 1], z_peer(k)).wait_recv()
        acc = acc + modz[k - 1]
    modf[tp] = acc
    for k in range(1, TP):
        send(modf.at[tp], modf.at[tp], ts.at[k - 1], tr.at[k - 1], t_peer(k))

    halo_up.wait_recv()
    send(hbuf.at[0, half], hbuf.at[0, half], hps.at[0], hpr.at[0], at(sp, partner))
    halo_dn.wait_recv()
    send(hbuf.at[1, half], hbuf.at[1, half], hps.at[1], hpr.at[1], at(sp, partner))

    for k in range(1, TP):
        remote(cbuf.at[tp], cbuf.at[tp], cts.at[k - 1], ctr.at[k - 1], t_peer(k)).wait_recv()
    for zz in range(Z):
        for g in range(TP):
            cf[4 * zz : 4 * zz + 4, g * F : (g + 1) * F] = cbuf[g, zz].astype(jnp.float32)

    def store_ctx(r, v):
        cf[r, :] = v

    normed(lambda r: cf[r, :], store_ctx, 64, 16)

    for s in range(2):
        remote(hbuf.at[s, half], hbuf.at[s, half], hps.at[s], hpr.at[s], at(sp, partner)).wait_recv()

        def store_halo(r, v, s=s):
            xn[2 * s, r, :] = v

        normed(lambda r, s=s: hbuf[s, r, :], store_halo, TOK, 16)

    lo, hi = pl.ds(0, 64), pl.ds(64, 64)
    w_right.wait_recv()
    send(wfull.at[left, lo], wfull.at[left, lo], ws.at[2], wr.at[2], at(sp, right))
    send(wfull.at[left], wfull.at[left], wps.at[1], wpr.at[1], at(sp, partner))
    w_left.wait_recv()
    send(wfull.at[right, hi], wfull.at[right, hi], ws.at[3], wr.at[3], at(sp, left))
    send(wfull.at[right], wfull.at[right], wps.at[2], wpr.at[2], at(sp, partner))

    for k in range(1, TP):
        remote(modf.at[tp], modf.at[tp], ts.at[k - 1], tr.at[k - 1], t_peer(k)).wait_recv()

    own_k.wait()
    own_v.wait()
    own_q.wait()
    lane = lax.broadcasted_iota(jnp.int32, (1, 128), 1)
    qg2 = jnp.concatenate([qg[...], qg[...]], axis=1)
    kg2 = jnp.concatenate([kg[...], kg[...]], axis=1)

    for g in range(TP):
        gs = slice(g * F, (g + 1) * F)
        hid[0:64, gs] = (cf[:, gs] * (1.0 + modf[g, 3:4, :]) + modf[g, 1:2, :]).astype(jnp.bfloat16)
    kv = jnp.dot(hid[0:64, :], wkvv[...], preferred_element_type=jnp.float32)
    ckv[y, :, 0:128] = head_norm(kv[:, 0:128], kg2).astype(jnp.bfloat16)
    ckv[y, :, 128:256] = kv[:, 128:256].astype(jnp.bfloat16)
    for k in (4, 3, 5, 2, 6, 1, 7):
        send(ckv.at[y], ckv.at[y], cys.at[k - 1], cyr.at[k - 1], y_peer(k))

    for b in (1, 0, 2):
        def rows_step(n, carry, b=b):
            r = pl.ds(pl.multiple_of(n * 128, 128), 128)
            for g in range(TP):
                gs = slice(g * F, (g + 1) * F)
                hid[:, gs] = (xn[b, r, gs] * (1.0 + modf[g, 2:3, :]) + modf[g, 0:1, :]).astype(jnp.bfloat16)
            h = hid[...]
            kv = jnp.dot(h, wkvv[...], preferred_element_type=jnp.float32)
            kr = pl.ds(pl.multiple_of(b * TOK + n * 128, 128), 128)
            kpad[kr, :] = head_norm(kv[:, 0:128], kg2).astype(jnp.bfloat16)
            vpad[kr, :] = kv[:, 128:256].astype(jnp.bfloat16)
            if b == 1:
                q = jnp.dot(h, wqv[...], preferred_element_type=jnp.float32)
                q = (head_norm(q, qg2) * (HD**-0.5)).astype(jnp.bfloat16)
                zero = jnp.zeros_like(q)
                lf = jnp.broadcast_to(lane < HD, q.shape)
                q0 = jnp.where(lf, q, zero)
                q1 = jnp.where(lf, zero, q)
                for i in range(2):
                    q2[2 * n + i, 0:64, :] = q0[i * 64 : (i + 1) * 64]
                    q2[2 * n + i, 64:128, :] = q1[i * 64 : (i + 1) * 64]
            return carry

        lax.fori_loop(0, 2, rows_step, 0)

    nt = (((1,), (1,)), ((), ()))
    at_first = sp == 0
    at_last = sp == SP - 1
    m_w, l_w, band = [], [], []
    for i in range(ROWS):
        start = jnp.where(at_first, 4, jnp.where(at_last, 0, i))
        off = jnp.where(at_first, 7 - i, 3 + jnp.where(at_last, -i, 0))
        rows = pl.ds(pl.multiple_of(start * COLS, COLS), 8 * COLS)
        band.append(rows)
        s = lax.dot_general(q2[i], kpad[rows, :], nt, preferred_element_type=jnp.float32)
        tiles = []
        for p in range(4):
            t = jnp.concatenate([tbl[0, off + 2 * p], tbl[1, off + 2 * p]], axis=0)
            tiles.append(s[:, p * 128 : (p + 1) * 128] + t)
        s = jnp.concatenate(tiles, axis=1)
        m = jnp.max(s, axis=1, keepdims=True)
        e = jnp.exp(s - m)
        ew[i] = e
        m_w.append(m)
        l_w.append(jnp.sum(e, axis=1, keepdims=True))

    remote(wfull.at[left, lo], wfull.at[far, lo], ws.at[2], wr.at[2], at(sp, right)).wait_recv()
    remote(wfull.at[right, hi], wfull.at[far, hi], ws.at[3], wr.at[3], at(sp, left)).wait_recv()
    send(wfull.at[far], wfull.at[far], wps.at[3], wpr.at[3], at(sp, partner))

    for k in range(1, Y):
        remote(ckv.at[y], ckv.at[y], cys.at[k - 1], cyr.at[k - 1], y_peer(k)).wait_recv()
    ck = ckv[:, :, 0:128].reshape(512, 128)
    cv = ckv[:, :, 128:256].reshape(512, 128)
    for i in range(ROWS):
        sc = lax.dot_general(q2[i], ck, nt, preferred_element_type=jnp.float32)
        m = jnp.maximum(m_w[i], jnp.max(sc, axis=1, keepdims=True))
        ec = jnp.exp(sc - m)
        fw = jnp.exp(m_w[i] - m)
        inv = 1.0 / (l_w[i] * fw + jnp.sum(ec, axis=1, keepdims=True))
        w_win = (ew[i] * (fw * inv)).astype(jnp.bfloat16)
        w_ctx = (ec * inv).astype(jnp.bfloat16)
        o = jnp.dot(w_win, vpad[band[i], :], preferred_element_type=jnp.float32) + jnp.dot(
            w_ctx, cv, preferred_element_type=jnp.float32
        )
        o = jnp.where(jnp.broadcast_to(lane < HD, (64, 128)), o[0:64], o[64:128])
        attb[tp, i * COLS : (i + 1) * COLS, :] = o.astype(jnp.bfloat16)
    for k in (4, 2, 6, 3, 5, 1, 7):
        send(attb.at[tp], attb.at[tp], as_.at[k - 1], ar.at[k - 1], t_peer(k))

    for k in range(1, TP):
        remote(attb.at[tp], attb.at[tp], as_.at[k - 1], ar.at[k - 1], t_peer(k)).wait_recv()
    for n in range(4):
        remote(wfull.at[tp], wfull.at[tp], wps.at[n], wpr.at[n], at(sp, partner)).wait_recv()

    def out_copy(n):
        cols = pl.ds(pl.multiple_of(n * F, F), F)
        return pltpu.make_async_copy(outv.at[:, cols], out.at[:, cols], out_sem.at[n])

    def proj_step(n, carry):
        cols = pl.ds(pl.multiple_of(n * F, F), F)
        acc = jnp.zeros((TOK, F), jnp.float32)
        for g in range(TP):
            t = jnp.dot(attb[g], wfull[g, :, cols], preferred_element_type=jnp.float32)
            acc = acc + t.astype(jnp.bfloat16).astype(jnp.float32)
        res = latv[:, cols].astype(jnp.float32) + modf[n, 4:5, :] * acc
        outv[:, cols] = res.astype(jnp.bfloat16)
        out_copy(n).start()
        return carry

    lax.fori_loop(0, TP, proj_step, 0)

    for d in sends:
        d.wait_send()
    for n in range(TP):
        out_copy(n).wait()


def per_device(latent, context, cond, cctx, shw, scw, gw, gain, wq, wk, wv, qg, kg, bias, outw):
    any_ = pl.BlockSpec(memory_space=pl.ANY)
    vm = pl.BlockSpec(memory_space=pltpu.VMEM)
    sm = pl.BlockSpec(memory_space=pltpu.SMEM)
    bf, f32 = jnp.bfloat16, jnp.float32
    dma = pltpu.SemaphoreType.DMA
    scratch = [
        pltpu.VMEM((5, F), f32),
        pltpu.VMEM((Y - 1, 5, F), f32),
        pltpu.VMEM((5, F), f32),
        pltpu.VMEM((Z - 1, 5, F), f32),
        pltpu.VMEM((TP, 5, F), f32),
        pltpu.VMEM((TP, Z, 4, F), bf),
        pltpu.VMEM((64, D), f32),
        pltpu.VMEM((Y, 64, 256), bf),
        pltpu.VMEM((2, TOK, D), bf),
        pltpu.VMEM((3, TOK, D), f32),
        pltpu.VMEM((128, D), bf),
        pltpu.VMEM((D, 128), bf),
        pltpu.VMEM((D, 256), bf),
        pltpu.VMEM((TP, 128, D), bf),
        pltpu.VMEM((TOK, D), bf),
        pltpu.VMEM((2, 14, COLS, 128), f32),
        pltpu.VMEM((3 * TOK, 128), bf),
        pltpu.VMEM((3 * TOK, 128), bf),
        pltpu.VMEM((ROWS, 128, 128), bf),
        pltpu.VMEM((ROWS, 128, 512), f32),
        pltpu.VMEM((TP, TOK, 128), bf),
        pltpu.VMEM((TOK, D), bf),
        dma((6,)),
        dma((TP,)),
    ]
    for n in (7, 7, 15, 15, 7, 7, 15, 15, 7, 7, 7, 7, 2, 2, 2, 2, 4, 4, 4, 4, 7, 7):
        scratch.append(dma((n,)))
    return pl.pallas_call(
        kernel,
        out_shape=jax.ShapeDtypeStruct((TOK, D), bf),
        in_specs=[any_, any_, vm, vm, vm, vm, vm, vm, any_, any_, any_, vm, vm, sm, any_],
        out_specs=any_,
        scratch_shapes=scratch,
        compiler_params=pltpu.CompilerParams(
            collective_id=0, has_side_effects=True, vmem_limit_bytes=56 * 1024 * 1024
        ),
        name="fused",
    )(
        latent, context, cond.reshape(1, 16), cctx.reshape(1, 16), shw, scw, gw, gain.reshape(1, D),
        wq, wk, wv, qg.reshape(1, HD), kg.reshape(1, HD), bias, outw,
    )


def solution(mesh):
    placed = (
        P("sp", None), P("sp", None), P("sp"), P("sp"),
        P("sp", "tp"), P("sp", "tp"), P("sp", "tp"), P(),
        P(None, "tp"), P(None, "tp"), P(None, "tp"), P(), P(),
        P("tp", None, None), P("tp", None),
    )
    return jax.shard_map(
        per_device, mesh=mesh, in_specs=placed, out_specs=P("sp", None), check_vma=False
    )
```

```python
import jax
import jax.numpy as jnp
from jax import lax
from jax.experimental import pallas as pl
from jax.experimental.pallas import tpu as pltpu
from jax.sharding import PartitionSpec as P

MESH = pl.DeviceIdType.MESH
EPS = 1e-06
Z, Y, TP = 16, 8, 8
SP = Z * Y
D = 2048
F = D // TP
TOK = 256
COLS = 64
ROWS = 4
HD = 64
HALF = D // 2
NEG = float("-inf")


def rem(a, n):
    return lax.rem(a, jnp.int32(n))


def head_norm(p, gain2):
    lane = lax.broadcasted_iota(jnp.int32, p.shape, 1)
    left = lane < HD
    sq = p * p
    s0 = jnp.sum(jnp.where(left, sq, 0.0), axis=1, keepdims=True)
    s1 = jnp.sum(jnp.where(left, 0.0, sq), axis=1, keepdims=True)
    r0 = lax.rsqrt(s0 * (1.0 / HD) + EPS)
    r1 = lax.rsqrt(s1 * (1.0 / HD) + EPS)
    return p * jnp.where(left, r0, r1) * gain2


def kernel(
    latent, context, cond_h, cctx_h, shw_h, scw_h, gw_h, gain_h, wq, wk, wv, qg_h, kg_h, bias_h, outw,
    out,
    cond, cctx, shw, scw, gw, gain, qg, kg, bias,
    part, mody, zpart, modz, modf,
    cbuf, cf, ckv,
    xn, hid, chid,
    wqv, wkvv, wfull, latv,
    tbl, kvp, q2, ec, attb, orem,
    small_sem, loc_sem,
    ys, yr, zs, zr, ts, tr,
    czs, czr, cts, ctr, cps, cpr, cys, cyr,
    hs, hr, ws, wr, fs, fr,
    as_, ar, aps, apr, os_, or_,
):
    sp = lax.axis_index("sp")
    tp = lax.axis_index("tp")
    y = rem(sp, Y)
    z = lax.div(sp, jnp.int32(Y))
    c = rem(tp, 2)
    mate = y + 1 - 2 * rem(y, 2)
    side = 2 * rem(y, 2) - 1
    pair = lax.div(y, jnp.int32(2))
    partner = tp + 1 - 2 * c
    up = rem(sp + 1, SP)
    down = rem(sp + SP - 1, SP)
    right = rem(tp + 2, TP)
    left = rem(tp + TP - 2, TP)
    far = rem(tp + 4, TP)

    def at(s, t):
        return {"sp": s, "tp": t}

    def y_peer(k):
        return at(z * Y + rem(y + k, Y), tp)

    def z_peer(k):
        return at(rem(z + k, Z) * Y + y, tp)

    def m_peer(k):
        return at(rem(z + k, Z) * Y + mate, tp)

    def t_peer(k):
        return at(sp, rem(tp + k, TP))

    def remote(src, dst, s, r, dev):
        return pltpu.make_async_remote_copy(
            src_ref=src, dst_ref=dst, send_sem=s, recv_sem=r, device_id=dev, device_id_type=MESH
        )

    sends = []

    def send(src, dst, s, r, dev):
        d = remote(src, dst, s, r, dev)
        d.start()
        sends.append(d)
        return d

    small = [
        pltpu.make_async_copy(src, dst, small_sem.at[n])
        for n, (src, dst) in enumerate(
            (
                (cond_h, cond), (cctx_h, cctx), (shw_h, shw), (scw_h, scw), (gw_h, gw),
                (bias_h, bias), (gain_h, gain), (qg_h, qg), (kg_h, kg),
            )
        )
    ]
    for d in small:
        d.start()
    ctx_col = pl.multiple_of(tp * F, F)
    my_half = pl.ds(pl.multiple_of(c * HALF, HALF), HALF)
    its_half = pl.ds(pl.multiple_of((1 - c) * HALF, HALF), HALF)
    own_ctx = cbuf.at[tp, y - 2 * pair, z]
    own_c = pltpu.make_async_copy(context.at[:, pl.ds(ctx_col, F)], own_ctx, loc_sem.at[0])
    own_l = pltpu.make_async_copy(latent, latv, loc_sem.at[1])
    own_q = pltpu.make_async_copy(wq, wqv, loc_sem.at[2])
    own_k = pltpu.make_async_copy(wk, wkvv.at[:, pl.ds(0, 128)], loc_sem.at[3])
    own_v = pltpu.make_async_copy(wv, wkvv.at[:, pl.ds(128, 128)], loc_sem.at[4])
    own_w = pltpu.make_async_copy(outw.at[:, my_half], wfull.at[tp], loc_sem.at[5])
    own_c.start()
    own_l.start()
    own_q.start()
    own_k.start()
    own_v.start()
    own_w.start()

    barrier = pltpu.get_barrier_semaphore()
    z_order = (8, 7, 9, 6, 10, 5, 11, 4, 12, 3, 13, 2, 14, 1, 15)
    y_order = (4, 3, 5, 2, 6, 1, 7)
    peers = [z_peer(k) for k in z_order] + [m_peer(k) for k in z_order + (0,)]
    peers += [y_peer(k) for k in y_order]
    peers += [t_peer(k) for k in range(1, TP)]
    peers += [at(up, tp), at(down, tp)]
    for p in peers:
        pl.semaphore_signal(barrier, inc=1, device_id=p, device_id_type=MESH)

    for d in small:
        d.wait()
    row8 = lax.broadcasted_iota(jnp.int32, (8, 16), 0)
    pre = jnp.where(row8 == 0, jnp.broadcast_to(cond[...], (8, 16)), jnp.broadcast_to(cctx[...], (8, 16)))
    act = (pre / (1.0 + jnp.exp(-pre))).astype(jnp.bfloat16)
    p_sh = jnp.dot(act, shw[...], preferred_element_type=jnp.float32)
    p_sc = jnp.dot(act, scw[...], preferred_element_type=jnp.float32)
    p_g = jnp.dot(act, gw[...], preferred_element_type=jnp.float32)
    part[0:2, :] = p_sh[0:2]
    part[2:4, :] = p_sc[0:2]
    part[4:5, :] = p_g[0:1]
    own_c.wait()

    pl.semaphore_wait(barrier, len(peers))

    for k in y_order:
        send(part, mody.at[k - 1], ys.at[k - 1], yr.at[k - 1], y_peer(k))
    for k in z_order:
        send(own_ctx, own_ctx, czs.at[k], czr.at[k], z_peer(k))
        send(own_ctx, own_ctx, czs.at[Z + k], czr.at[Z + k], m_peer(k))
    send(own_ctx, own_ctx, czs.at[Z], czr.at[Z], m_peer(0))
    send(outw.at[:, its_half], wfull.at[tp], ws.at[0], wr.at[0], at(sp, partner))
    send(outw.at[:, my_half], wfull.at[tp], ws.at[1], wr.at[1], at(sp, right))
    send(outw.at[:, my_half], wfull.at[tp], ws.at[2], wr.at[2], at(sp, left))

    tq = lax.broadcasted_iota(jnp.int32, (COLS, 128), 0)
    tl = lax.broadcasted_iota(jnp.int32, (COLS, 128), 1)
    tk = jnp.where(tl < COLS, tl, tl - COLS)
    diff = tk - tq + 15
    c0 = jnp.clip(tq - 8, 0, 48)
    is_open = (tk >= c0) & (tk < c0 + 16)
    first = lax.broadcasted_iota(jnp.int32, (1, 128), 1) < COLS

    def table_step(n, carry):
        h = lax.div(n, jnp.int32(14))
        a = rem(n, 14)
        val = jnp.full((COLS, 128), NEG, jnp.float32)
        for dd in range(31):
            v = jnp.where(first, bias[a, h, dd], bias[a + 1, h, dd])
            val = jnp.where(diff == dd, jnp.broadcast_to(v, (COLS, 128)), val)
        tbl[h, a] = jnp.where(is_open, val, NEG)
        return carry

    lax.fori_loop(0, 28, table_step, 0)

    def normed(load, store, rows, chunk):
        def step(n, carry):
            r = pl.ds(pl.multiple_of(n * chunk, chunk), chunk)
            v = load(r).astype(jnp.float32)
            ms = jnp.mean(v * v, axis=-1, keepdims=True)
            store(r, v * lax.rsqrt(ms + EPS) * gain[...])
            return carry

        lax.fori_loop(0, rows // chunk, step, 0)

    acc = part[...]
    for k in range(1, Y):
        remote(part, mody.at[k - 1], ys.at[k - 1], yr.at[k - 1], y_peer(k)).wait_recv()
        acc = acc + mody[k - 1]
    zpart[...] = acc
    for k in z_order:
        send(zpart, modz.at[k - 1], zs.at[k - 1], zr.at[k - 1], z_peer(k))

    own_l.wait()

    def store_own(r, v):
        xn[r, :] = v

    normed(lambda r: latv[r, :], store_own, TOK, 16)

    for k in z_order:
        remote(own_ctx, own_ctx, czs.at[k], czr.at[k], z_peer(k)).wait_recv()
    for k in z_order + (0,):
        remote(own_ctx, own_ctx, czs.at[Z + k], czr.at[Z + k], m_peer(k)).wait_recv()
    hops = ((far, 0), (right, 1), (left, 2), (partner, 3))
    for t, n in hops:
        send(cbuf.at[tp], cbuf.at[tp], cts.at[n], ctr.at[n], at(sp, t))

    acc = zpart[...]
    for k in range(1, Z):
        remote(zpart, modz.at[k - 1], zs.at[k - 1], zr.at[k - 1], z_peer(k)).wait_recv()
        acc = acc + modz[k - 1]
    modf[tp] = acc
    for k in (4, 3, 5, 2, 6, 1, 7):
        send(modf.at[tp], modf.at[tp], ts.at[k - 1], tr.at[k - 1], t_peer(k))

    for t, n, frm in ((right, 1, left), (left, 2, right), (far, 0, far)):
        remote(cbuf.at[tp], cbuf.at[tp], cts.at[n], ctr.at[n], at(sp, t)).wait_recv()
        send(cbuf.at[frm], cbuf.at[frm], cps.at[n], cpr.at[n], at(sp, partner))
    remote(cbuf.at[tp], cbuf.at[tp], cts.at[3], ctr.at[3], at(sp, partner)).wait_recv()
    for n in range(3):
        remote(cbuf.at[tp], cbuf.at[tp], cps.at[n], cpr.at[n], at(sp, partner)).wait_recv()

    for j in range(2 * Z):
        for g in range(TP):
            cf[4 * j : 4 * j + 4, g * F : (g + 1) * F] = cbuf[g, j % 2, j // 2].astype(jnp.float32)

    def store_ctx(r, v):
        cf[r, :] = v

    normed(lambda r: cf[r, :], store_ctx, 128, 16)

    for k in range(1, TP):
        remote(modf.at[tp], modf.at[tp], ts.at[k - 1], tr.at[k - 1], t_peer(k)).wait_recv()

    own_k.wait()
    own_v.wait()
    own_q.wait()
    lane = lax.broadcasted_iota(jnp.int32, (1, 128), 1)
    qg2 = jnp.concatenate([qg[...], qg[...]], axis=1)
    kg2 = jnp.concatenate([kg[...], kg[...]], axis=1)

    for g in range(TP):
        gs = slice(g * F, (g + 1) * F)
        chid[:, gs] = (cf[:, gs] * (1.0 + modf[g, 3:4, :]) + modf[g, 1:2, :]).astype(jnp.bfloat16)
    kv = jnp.dot(chid[...], wkvv[...], preferred_element_type=jnp.float32)
    ckv[pair, :, 0:128] = head_norm(kv[:, 0:128], kg2).astype(jnp.bfloat16)
    ckv[pair, :, 128:256] = kv[:, 128:256].astype(jnp.bfloat16)
    own_pair = ckv.at[pair]
    for k in (3, 2, 1):
        send(own_pair, own_pair, cys.at[k - 1], cyr.at[k - 1], at(z * Y + rem(y + side * k + Y, Y), tp))

    lo, hi = pl.ds(0, 64), pl.ds(64, 64)

    def w_wait(n, t):
        remote(wfull.at[tp], wfull.at[tp], ws.at[n], wr.at[n], at(sp, t)).wait_recv()

    def w_forward(n, frm_left, frm_right):
        send(wfull.at[frm_left, lo], wfull.at[frm_left, lo], fs.at[n], fr.at[n], at(sp, right))
        send(wfull.at[frm_right, hi], wfull.at[frm_right, hi], fs.at[n + 1], fr.at[n + 1], at(sp, left))

    def other(t):
        return t + 1 - 2 * c

    send(outw.at[:, its_half], wfull.at[tp], ws.at[3], wr.at[3], at(sp, other(right)))
    send(outw.at[:, its_half], wfull.at[tp], ws.at[4], wr.at[4], at(sp, other(left)))
    w_wait(1, right)
    w_wait(2, left)
    w_forward(0, left, right)

    for n in range(2):
        r = pl.ds(n * 128, 128)
        for g in range(TP):
            gs = slice(g * F, (g + 1) * F)
            hid[r, gs] = (xn[r, gs] * (1.0 + modf[g, 2:3, :]) + modf[g, 0:1, :]).astype(jnp.bfloat16)
        h = hid[r, :]
        kv = jnp.dot(h, wkvv[...], preferred_element_type=jnp.float32)
        kr = pl.ds(TOK + n * 128, 128)
        kvp[kr, 0:128] = head_norm(kv[:, 0:128], kg2).astype(jnp.bfloat16)
        kvp[kr, 128:256] = kv[:, 128:256].astype(jnp.bfloat16)
    own_rows = kvp.at[pl.ds(TOK, TOK)]
    send(own_rows, kvp.at[pl.ds(0, TOK)], hs.at[0], hr.at[0], at(up, tp))
    send(own_rows, kvp.at[pl.ds(2 * TOK, TOK)], hs.at[1], hr.at[1], at(down, tp))
    for n in range(2):
        r = pl.ds(n * 128, 128)
        q = jnp.dot(hid[r, :], wqv[...], preferred_element_type=jnp.float32)
        q = (head_norm(q, qg2) * (HD**-0.5)).astype(jnp.bfloat16)
        zero = jnp.zeros_like(q)
        lf = jnp.broadcast_to(lane < HD, q.shape)
        q0 = jnp.where(lf, q, zero)
        q1 = jnp.where(lf, zero, q)
        for i in range(2):
            q2[2 * n + i, 0:64, :] = q0[i * 64 : (i + 1) * 64]
            q2[2 * n + i, 64:128, :] = q1[i * 64 : (i + 1) * 64]

    w_wait(3, other(right))
    w_wait(4, other(left))
    w_forward(2, other(left), other(right))

    nt = (((1,), (1,)), ((), ()))
    for k in (1, 2, 3):
        remote(own_pair, own_pair, cys.at[k - 1], cyr.at[k - 1], at(z * Y + mate, tp)).wait_recv()
    ck = ckv[:, :, 0:128].reshape(512, 128)
    m_c, l_c = [], []
    for i in range(ROWS):
        s = lax.dot_general(q2[i], ck, nt, preferred_element_type=jnp.float32)
        m = jnp.max(s, axis=1, keepdims=True)
        e = jnp.exp(s - m)
        ec[i] = e
        m_c.append(m)
        l_c.append(jnp.sum(e, axis=1, keepdims=True))

    for n in range(2):
        remote(own_rows, kvp.at[pl.ds(0, TOK)], hs.at[n], hr.at[n], at(up, tp)).wait_recv()

    at_first = sp == 0
    at_last = sp == SP - 1
    cv = ckv[:, :, 128:256].reshape(512, 128)
    for i in range(ROWS):
        start = jnp.where(at_first, 4, jnp.where(at_last, 0, i))
        off = jnp.where(at_first, 7 - i, 3 + jnp.where(at_last, -i, 0))
        rows = pl.ds(pl.multiple_of(start * COLS, COLS), 8 * COLS)
        s = lax.dot_general(q2[i], kvp[rows, 0:128], nt, preferred_element_type=jnp.float32)
        tiles = []
        for p in range(4):
            t = jnp.concatenate([tbl[0, off + 2 * p], tbl[1, off + 2 * p]], axis=0)
            tiles.append(s[:, p * 128 : (p + 1) * 128] + t)
        s = jnp.concatenate(tiles, axis=1)
        m = jnp.maximum(m_c[i], jnp.max(s, axis=1, keepdims=True))
        ew = jnp.exp(s - m)
        fc = jnp.exp(m_c[i] - m)
        inv = 1.0 / (l_c[i] * fc + jnp.sum(ew, axis=1, keepdims=True))
        w_win = (ew * inv).astype(jnp.bfloat16)
        w_ctx = (ec[i] * (fc * inv)).astype(jnp.bfloat16)
        o = jnp.dot(w_win, kvp[rows, 128:256], preferred_element_type=jnp.float32) + jnp.dot(
            w_ctx, cv, preferred_element_type=jnp.float32
        )
        o = jnp.where(jnp.broadcast_to(lane < HD, (64, 128)), o[0:64], o[64:128])
        attb[tp, i * COLS : (i + 1) * COLS, :] = o.astype(jnp.bfloat16)
        if i % 2 == 1:
            hh = i // 2
            block = attb.at[tp, pl.ds(hh * 128, 128)]
            for t, n in hops:
                send(block, block, as_.at[hh * 4 + n], ar.at[hh * 4 + n], at(sp, t))

    for hh in range(2):
        rr = pl.ds(hh * 128, 128)
        block = attb.at[tp, rr]
        for t, n, frm in ((right, 1, left), (left, 2, right), (far, 0, far)):
            remote(block, block, as_.at[hh * 4 + n], ar.at[hh * 4 + n], at(sp, t)).wait_recv()
            b = attb.at[frm, rr]
            send(b, b, aps.at[hh * 3 + n], apr.at[hh * 3 + n], at(sp, partner))

    w_wait(0, partner)
    own_w.wait()
    for n in range(4):
        remote(wfull.at[left, lo], wfull.at[far, lo], fs.at[n], fr.at[n], at(sp, right)).wait_recv()

    for hh in range(2):
        rr = pl.ds(hh * 128, 128)
        block = attb.at[tp, rr]
        remote(block, block, as_.at[hh * 4 + 3], ar.at[hh * 4 + 3], at(sp, partner)).wait_recv()
        for n in range(3):
            remote(block, block, aps.at[hh * 3 + n], apr.at[hh * 3 + n], at(sp, partner)).wait_recv()
        for n in range(HALF // F):
            cols = pl.ds(pl.multiple_of(c * HALF + n * F, F), F)
            acc = jnp.zeros((128, F), jnp.float32)
            for g in range(TP):
                t = jnp.dot(attb[g, rr, :], wfull[g, :, n * F : (n + 1) * F], preferred_element_type=jnp.float32)
                acc = acc + t.astype(jnp.bfloat16).astype(jnp.float32)
            res = latv[rr, cols].astype(jnp.float32) + modf[c * (HALF // F) + n, 4:5, :] * acc
            out[rr, cols] = res.astype(jnp.bfloat16)
        send(out.at[rr, my_half], orem.at[rr], os_.at[hh], or_.at[hh], at(sp, partner))
    for hh in range(2):
        rr = pl.ds(hh * 128, 128)
        remote(orem.at[rr], orem.at[rr], os_.at[hh], or_.at[hh], at(sp, partner)).wait_recv()
        out[rr, its_half] = orem[rr, :]

    for d in sends:
        d.wait_send()


def per_device(latent, context, cond, cctx, shw, scw, gw, gain, wq, wk, wv, qg, kg, bias, outw):
    hbm = pl.BlockSpec(memory_space=pltpu.HBM)
    vm = pl.BlockSpec(memory_space=pltpu.VMEM)
    bf, f32 = jnp.bfloat16, jnp.float32
    dma = pltpu.SemaphoreType.DMA
    scratch = [
        pltpu.VMEM((1, 16), f32),
        pltpu.VMEM((1, 16), f32),
        pltpu.VMEM((16, F), bf),
        pltpu.VMEM((16, F), bf),
        pltpu.VMEM((16, F), bf),
        pltpu.VMEM((1, D), f32),
        pltpu.VMEM((1, HD), f32),
        pltpu.VMEM((1, HD), f32),
        pltpu.SMEM((15, 2, 31), f32),
        pltpu.VMEM((5, F), f32),
        pltpu.VMEM((Y - 1, 5, F), f32),
        pltpu.VMEM((5, F), f32),
        pltpu.VMEM((Z - 1, 5, F), f32),
        pltpu.VMEM((TP, 5, F), f32),
        pltpu.VMEM((TP, 2, Z, 4, F), bf),
        pltpu.VMEM((128, D), f32),
        pltpu.VMEM((4, 128, 256), bf),
        pltpu.VMEM((TOK, D), f32),
        pltpu.VMEM((TOK, D), bf),
        pltpu.VMEM((128, D), bf),
        pltpu.VMEM((D, 128), bf),
        pltpu.VMEM((D, 256), bf),
        pltpu.VMEM((TP, 128, HALF), bf),
        pltpu.VMEM((TOK, D), bf),
        pltpu.VMEM((2, 14, COLS, 128), f32),
        pltpu.VMEM((3 * TOK, 256), bf),
        pltpu.VMEM((ROWS, 128, 128), bf),
        pltpu.VMEM((ROWS, 128, 512), f32),
        pltpu.VMEM((TP, TOK, 128), bf),
        pltpu.VMEM((TOK, HALF), bf),
        dma((9,)),
        dma((6,)),
    ]
    for n in (7, 15, 7, 32, 4, 3, 3, 2, 5, 4, 8, 6, 2):
        scratch += [dma((n,)), dma((n,))]
    return pl.pallas_call(
        kernel,
        out_shape=jax.ShapeDtypeStruct((TOK, D), bf),
        in_specs=[hbm] * 15,
        out_specs=vm,
        scratch_shapes=scratch,
        compiler_params=pltpu.CompilerParams(
            collective_id=0, has_side_effects=True, vmem_limit_bytes=40 * 1024 * 1024
        ),
        name="fused",
    )(
        *(
            pltpu.with_memory_space_constraint(a, pltpu.HBM)
            for a in (
                latent, context, cond.reshape(1, 16), cctx.reshape(1, 16), shw, scw, gw, gain.reshape(1, D),
                wq, wk, wv, qg.reshape(1, HD), kg.reshape(1, HD), bias.transpose(1, 0, 2), outw,
            )
        )
    )


def solution(mesh):
    placed = (
        P("sp", None), P("sp", None), P("sp"), P("sp"),
        P("sp", "tp"), P("sp", "tp"), P("sp", "tp"), P(),
        P(None, "tp"), P(None, "tp"), P(None, "tp"), P(), P(),
        P("tp", None, None), P("tp", None),
    )
    return jax.shard_map(
        per_device, mesh=mesh, in_specs=placed, out_specs=P("sp", None), check_vma=False
    )
```

```python
import jax
import jax.numpy as jnp
from jax import lax
from jax.experimental import pallas as pl
from jax.experimental.pallas import tpu as pltpu
from jax.sharding import PartitionSpec as P

MESH = pl.DeviceIdType.MESH
EPS = 1e-06
Z, Y, TP = 16, 8, 8
SP = Z * Y
D = 2048
F = D // TP
TOK = 256
COLS = 64
ROWS = 4
HD = 64
HALF = D // 2
NEG = float("-inf")


def rem(a, n):
    return lax.rem(a, jnp.int32(n))


def head_norm(p, gain2):
    lane = lax.broadcasted_iota(jnp.int32, p.shape, 1)
    left = lane < HD
    sq = p * p
    s0 = jnp.sum(jnp.where(left, sq, 0.0), axis=1, keepdims=True)
    s1 = jnp.sum(jnp.where(left, 0.0, sq), axis=1, keepdims=True)
    r0 = lax.rsqrt(s0 * (1.0 / HD) + EPS)
    r1 = lax.rsqrt(s1 * (1.0 / HD) + EPS)
    return p * jnp.where(left, r0, r1) * gain2


def kernel(
    latent, context, cond_h, cctx_h, shw_h, scw_h, gw_h, gain_h, wq, wk, wv, qg_h, kg_h, bias_h, outw,
    out,
    cc, modw, gain, qkg, bias,
    part, mody, zpart, modz, modf,
    cbuf, cf, ckv,
    xn, hid, chid,
    wall, wfull, latv,
    tbl, kvp, q2, ew, attb,
    relay, small_sem, loc_sem,
    ys, yr, zs, zr, ts, tr,
    czs, czr, cts, ctr, cpr, cys, cyr,
    hs, hr, ws, wr,
    as_, ar, apr, os_, or_,
):
    sp = lax.axis_index("sp")
    tp = lax.axis_index("tp")
    y = rem(sp, Y)
    z = lax.div(sp, jnp.int32(Y))
    c = rem(tp, 2)
    odd = rem(y, 2)
    mate = y + 1 - 2 * odd
    side = 2 * odd - 1
    pair = lax.div(y, jnp.int32(2))
    partner = tp + 1 - 2 * c
    up = rem(sp + 1, SP)
    down = rem(sp + SP - 1, SP)
    right = rem(tp + 2, TP)
    left = rem(tp + TP - 2, TP)
    far = rem(tp + 4, TP)

    def at(s, t):
        return {"sp": s, "tp": t}

    def y_peer(k):
        return at(z * Y + rem(y + k, Y), tp)

    def z_peer(k):
        return at(rem(z + k, Z) * Y + y, tp)

    def m_peer(k):
        return at(rem(z + k, Z) * Y + mate, tp)

    def t_peer(k):
        return at(sp, rem(tp + k, TP))

    def remote(src, dst, s, r, dev):
        return pltpu.make_async_remote_copy(
            src_ref=src, dst_ref=dst, send_sem=s, recv_sem=r, device_id=dev, device_id_type=MESH
        )

    def send(src, dst, s, r, dev):
        remote(src, dst, s, r, dev).start()

    def arrived(ref, r):
        remote(ref, ref, r, r, at(sp, partner)).wait_recv()

    def sent(ref, s):
        remote(ref, ref, s, s, at(sp, partner)).wait_send()

    barrier = pltpu.get_barrier_semaphore()
    near = (4, 12, 3, 13, 2, 14, 1, 15)
    beyond = (8, 7, 9, 6, 10, 5, 11)
    y_order = (4, 3, 5, 2, 6, 1, 7)
    peers = [y_peer(k) for k in y_order]
    peers += [z_peer(k) for k in near] + [m_peer(k) for k in near + (0,)]
    peers += [t_peer(k) for k in range(1, TP)]
    peers += [at(up, tp), at(down, tp)]
    for p in peers:
        pl.semaphore_signal(barrier, inc=1, device_id=p, device_id_type=MESH)

    small = (
        (cond_h, cc.at[0], 0), (cctx_h, cc.at[1], 0),
        (shw_h, modw.at[0], 1), (scw_h, modw.at[1], 1), (gw_h, modw.at[2], 1),
        (bias_h, bias, 2), (gain_h, gain, 3), (qg_h, qkg.at[0], 4), (kg_h, qkg.at[1], 4),
    )
    for src, dst, n in small:
        pltpu.make_async_copy(src, dst, small_sem.at[n]).start()
    ctx_col = pl.multiple_of(tp * F, F)
    my_half = pl.ds(pl.multiple_of(c * HALF, HALF), HALF)
    its_half = pl.ds(pl.multiple_of((1 - c) * HALF, HALF), HALF)
    own_ctx = cbuf.at[tp, odd, z]
    own_c = pltpu.make_async_copy(context.at[:, pl.ds(ctx_col, F)], own_ctx, loc_sem.at[0])
    own_l = pltpu.make_async_copy(latent, latv, loc_sem.at[1])
    own_w = pltpu.make_async_copy(outw.at[:, my_half], wfull.at[tp], loc_sem.at[2])
    own_c.start()
    own_l.start()
    own_w.start()
    for n, src in enumerate((wk, wv, wq)):
        pltpu.make_async_copy(src, wall.at[:, pl.ds(n * 128, 128)], loc_sem.at[3]).start()

    pl.semaphore_wait(barrier, len(peers))
    for k in (4, Z - 4):
        pl.semaphore_signal(relay, inc=1, device_id=z_peer(k), device_id_type=MESH)

    pltpu.make_async_copy(cc, cc, small_sem.at[0]).wait()
    pltpu.make_async_copy(modw, modw, small_sem.at[1]).wait()
    row8 = lax.broadcasted_iota(jnp.int32, (8, 16), 0)
    pre = jnp.where(row8 == 0, jnp.broadcast_to(cc[0], (8, 16)), jnp.broadcast_to(cc[1], (8, 16)))
    act = (pre / (1.0 + jnp.exp(-pre))).astype(jnp.bfloat16)
    p_sh = jnp.dot(act, modw[0], preferred_element_type=jnp.float32)
    p_sc = jnp.dot(act, modw[1], preferred_element_type=jnp.float32)
    p_g = jnp.dot(act, modw[2], preferred_element_type=jnp.float32)
    part[0:2, :] = p_sh[0:2]
    part[2:4, :] = p_sc[0:2]
    part[4:5, :] = p_g[0:1]

    def other(t):
        return t + 1 - 2 * c

    for k in y_order:
        send(part, mody.at[k - 1], ys, yr, y_peer(k))
    own_c.wait()
    for k in near:
        send(own_ctx, own_ctx, czs.at[0], czr.at[0], z_peer(k))
        send(own_ctx, own_ctx, czs.at[1], czr.at[1], m_peer(k))
    send(own_ctx, own_ctx, czs.at[1], czr.at[1], m_peer(0))
    send(outw.at[:, its_half], wfull.at[tp], ws, wr.at[0], at(sp, partner))
    send(outw.at[:, my_half], wfull.at[tp], ws, wr.at[1], at(sp, right))
    send(outw.at[:, my_half], wfull.at[tp], ws, wr.at[1], at(sp, left))
    send(outw.at[:, its_half], wfull.at[tp], ws, wr.at[2], at(sp, other(right)))
    send(outw.at[:, its_half], wfull.at[tp], ws, wr.at[2], at(sp, other(left)))

    pl.semaphore_wait(relay, 2)
    for k in beyond:
        send(own_ctx, own_ctx, czs.at[0], czr.at[0], z_peer(k))
        send(own_ctx, own_ctx, czs.at[1], czr.at[1], m_peer(k))

    arrived(mody, yr)
    acc = part[...]
    for k in range(1, Y):
        acc = acc + mody[k - 1]
    zpart[...] = acc
    for k in beyond + near:
        send(zpart, modz.at[k - 1], zs, zr, z_peer(k))

    tq = lax.broadcasted_iota(jnp.int32, (COLS, 128), 0)
    tl = lax.broadcasted_iota(jnp.int32, (COLS, 128), 1)
    tk = jnp.where(tl < COLS, tl, tl - COLS)
    diff = tk - tq + 15
    c0 = jnp.clip(tq - 8, 0, 48)
    is_open = (tk >= c0) & (tk < c0 + 16)
    first = lax.broadcasted_iota(jnp.int32, (1, 128), 1) < COLS

    def table_step(n, carry):
        h = lax.div(n, jnp.int32(14))
        a = rem(n, 14)
        val = jnp.full((COLS, 128), NEG, jnp.float32)
        for dd in range(31):
            v = jnp.where(first, bias[a, h, dd], bias[a + 1, h, dd])
            val = jnp.where(diff == dd, jnp.broadcast_to(v, (COLS, 128)), val)
        tbl[h, a] = jnp.where(is_open, val, NEG)
        return carry

    pltpu.make_async_copy(bias_h, bias, small_sem.at[2]).wait()
    lax.fori_loop(0, 28, table_step, 0)
    pltpu.make_async_copy(gain_h, gain, small_sem.at[3]).wait()

    def normed(load, store, rows, chunk):
        def step(n, carry):
            r = pl.ds(pl.multiple_of(n * chunk, chunk), chunk)
            v = load(r).astype(jnp.float32)
            ms = jnp.mean(v * v, axis=-1, keepdims=True)
            store(r, v * lax.rsqrt(ms + EPS) * gain[...])
            return carry

        lax.fori_loop(0, rows // chunk, step, 0)

    own_l.wait()

    def store_own(r, v):
        xn[r, :] = v

    normed(lambda r: latv[r, :], store_own, TOK, 16)

    arrived(cbuf.at[0, 0, pl.ds(0, Z - 1)], czr.at[0])
    arrived(cbuf.at[0, 0], czr.at[1])
    hops = ((far, 0), (right, 1), (left, 2), (partner, 3))
    for t, n in hops:
        send(cbuf.at[tp], cbuf.at[tp], cts, ctr.at[n], at(sp, t))

    arrived(modz, zr)
    acc = zpart[...]
    for k in range(1, Z):
        acc = acc + modz[k - 1]
    modf[tp] = acc
    for k in (4, 3, 5, 2, 6, 1, 7):
        send(modf.at[tp], modf.at[tp], ts, tr, t_peer(k))

    for n, frm in ((1, left), (2, right), (0, far)):
        arrived(cbuf.at[frm], ctr.at[n])
        send(cbuf.at[frm], cbuf.at[frm], cts, cpr, at(sp, partner))

    pltpu.make_async_copy(wall, wall, loc_sem.at[3]).wait()
    pltpu.make_async_copy(qkg, qkg, small_sem.at[4]).wait()
    arrived(modf.at[pl.ds(0, TP - 1)], tr)
    lane = lax.broadcasted_iota(jnp.int32, (1, 128), 1)
    qg2 = jnp.concatenate([qkg[0], qkg[0]], axis=1)
    kg2 = jnp.concatenate([qkg[1], qkg[1]], axis=1)

    for n in range(2):
        r = pl.ds(n * 128, 128)
        for g in range(TP):
            gs = slice(g * F, (g + 1) * F)
            hid[r, gs] = (xn[r, gs] * (1.0 + modf[g, 2:3, :]) + modf[g, 0:1, :]).astype(jnp.bfloat16)
        h = hid[r, :]
        kv = jnp.dot(h, wall[:, 0:256], preferred_element_type=jnp.float32)
        kr = pl.ds(TOK + n * 128, 128)
        kvp[kr, 0:128] = head_norm(kv[:, 0:128], kg2).astype(jnp.bfloat16)
        kvp[kr, 128:256] = kv[:, 128:256].astype(jnp.bfloat16)
    own_rows = kvp.at[pl.ds(TOK, TOK)]
    send(own_rows, kvp.at[pl.ds(0, TOK)], hs, hr, at(up, tp))
    send(own_rows, kvp.at[pl.ds(2 * TOK, TOK)], hs, hr, at(down, tp))

    arrived(cbuf.at[partner], ctr.at[3])
    arrived(cbuf.at[pl.ds(0, 3)], cpr)

    for j in range(2 * Z):
        for g in range(TP):
            cf[4 * j : 4 * j + 4, g * F : (g + 1) * F] = cbuf[g, j % 2, j // 2].astype(jnp.float32)

    def store_ctx(r, v):
        cf[r, :] = v

    normed(lambda r: cf[r, :], store_ctx, 128, 16)

    for g in range(TP):
        gs = slice(g * F, (g + 1) * F)
        chid[:, gs] = (cf[:, gs] * (1.0 + modf[g, 3:4, :]) + modf[g, 1:2, :]).astype(jnp.bfloat16)
    kv = jnp.dot(chid[...], wall[:, 0:256], preferred_element_type=jnp.float32)
    ckv[pair, :, 0:128] = head_norm(kv[:, 0:128], kg2).astype(jnp.bfloat16)
    ckv[pair, :, 128:256] = kv[:, 128:256].astype(jnp.bfloat16)
    own_pair = ckv.at[pair]
    send(own_pair, own_pair, cys, cyr.at[0], at(z * Y + rem(y + side + Y, Y), tp))
    send(own_pair, own_pair, cys, cyr.at[1], at(z * Y + rem(y + 3 * side + Y, Y), tp))

    for n in range(2):
        r = pl.ds(n * 128, 128)
        q = jnp.dot(hid[r, :], wall[:, 256:384], preferred_element_type=jnp.float32)
        q = (head_norm(q, qg2) * (HD**-0.5)).astype(jnp.bfloat16)
        zero = jnp.zeros_like(q)
        lf = jnp.broadcast_to(lane < HD, q.shape)
        q0 = jnp.where(lf, q, zero)
        q1 = jnp.where(lf, zero, q)
        for i in range(2):
            q2[2 * n + i, 0:64, :] = q0[i * 64 : (i + 1) * 64]
            q2[2 * n + i, 64:128, :] = q1[i * 64 : (i + 1) * 64]

    lo, hi = pl.ds(0, 64), pl.ds(64, 64)
    arrived(wfull.at[pl.ds(0, 2)], wr.at[1])
    arrived(wfull.at[pl.ds(0, 2)], wr.at[2])
    for f in (left, other(left)):
        send(wfull.at[f, lo], wfull.at[f, lo], ws, wr.at[3], at(sp, right))
    for f in (right, other(right)):
        send(wfull.at[f, hi], wfull.at[f, hi], ws, wr.at[3], at(sp, left))

    near_pair = ckv.at[rem(pair + side + 4, 4)]
    arrived(near_pair, cyr.at[0])
    send(near_pair, near_pair, cys, cyr.at[1], at(z * Y + mate, tp))

    arrived(kvp.at[pl.ds(0, 2 * TOK)], hr)

    nt = (((1,), (1,)), ((), ()))
    at_first = sp == 0
    at_last = sp == SP - 1
    m_w, l_w, band = [], [], []
    for i in range(ROWS):
        start = jnp.where(at_first, 4, jnp.where(at_last, 0, i))
        off = jnp.where(at_first, 7 - i, 3 + jnp.where(at_last, -i, 0))
        rows = pl.ds(pl.multiple_of(start * COLS, COLS), 8 * COLS)
        band.append(rows)
        s = lax.dot_general(q2[i], kvp[rows, 0:128], nt, preferred_element_type=jnp.float32)
        tiles = []
        for p in range(4):
            t = jnp.concatenate([tbl[0, off + 2 * p], tbl[1, off + 2 * p]], axis=0)
            tiles.append(s[:, p * 128 : (p + 1) * 128] + t)
        s = jnp.concatenate(tiles, axis=1)
        m = jnp.max(s, axis=1, keepdims=True)
        e = jnp.exp(s - m)
        ew[i] = e
        m_w.append(m)
        l_w.append(jnp.sum(e, axis=1, keepdims=True))

    arrived(ckv.at[pl.ds(0, 2)], cyr.at[1])

    ck = ckv[:, :, 0:128].reshape(512, 128)
    cv = ckv[:, :, 128:256].reshape(512, 128)
    for i in range(ROWS):
        s = lax.dot_general(q2[i], ck, nt, preferred_element_type=jnp.float32)
        m = jnp.maximum(m_w[i], jnp.max(s, axis=1, keepdims=True))
        ec = jnp.exp(s - m)
        fw = jnp.exp(m_w[i] - m)
        inv = 1.0 / (l_w[i] * fw + jnp.sum(ec, axis=1, keepdims=True))
        w_win = (ew[i] * (fw * inv)).astype(jnp.bfloat16)
        w_ctx = (ec * inv).astype(jnp.bfloat16)
        o = jnp.dot(w_win, kvp[band[i], 128:256], preferred_element_type=jnp.float32) + jnp.dot(
            w_ctx, cv, preferred_element_type=jnp.float32
        )
        o = jnp.where(jnp.broadcast_to(lane < HD, (64, 128)), o[0:64], o[64:128])
        attb[tp, i * COLS : (i + 1) * COLS, :] = o.astype(jnp.bfloat16)
        if i % 2 == 1:
            hh = i // 2
            block = attb.at[tp, pl.ds(hh * 128, 128)]
            for t, n in hops:
                send(block, block, as_, apr.at[hh] if n == 3 else ar.at[hh * 3 + n], at(sp, t))

    for hh in range(2):
        rr = pl.ds(hh * 128, 128)
        for n, frm in ((1, left), (2, right), (0, far)):
            block = attb.at[frm, rr]
            arrived(block, ar.at[hh * 3 + n])
            send(block, block, as_, apr.at[hh], at(sp, partner))

    arrived(wfull.at[partner], wr.at[0])
    own_w.wait()
    arrived(wfull.at[pl.ds(0, 2)], wr.at[3])

    for hh in range(2):
        rr = pl.ds(hh * 128, 128)
        arrived(attb.at[pl.ds(0, 2)], apr.at[hh])
        for n in range(HALF // F):
            cols = pl.ds(pl.multiple_of(c * HALF + n * F, F), F)
            acc = jnp.zeros((128, F), jnp.float32)
            for g in range(TP):
                t = jnp.dot(attb[g, rr, :], wfull[g, :, n * F : (n + 1) * F], preferred_element_type=jnp.float32)
                acc = acc + t.astype(jnp.bfloat16).astype(jnp.float32)
            res = latv[rr, cols].astype(jnp.float32) + modf[c * (HALF // F) + n, 4:5, :] * acc
            out[rr, cols] = res.astype(jnp.bfloat16)
            send(out.at[rr, cols], out.at[rr, cols], os_, or_, at(sp, partner))
    arrived(out.at[:, its_half], or_)

    sent(mody, ys)
    sent(modz, zs)
    sent(modf.at[pl.ds(0, TP - 1)], ts)
    sent(cbuf.at[0, 0, pl.ds(0, Z - 1)], czs.at[0])
    sent(cbuf.at[0, 0], czs.at[1])
    sent(cbuf.at[pl.ds(0, 7)], cts)
    sent(ckv.at[pl.ds(0, 3)], cys)
    sent(kvp.at[pl.ds(0, 2 * TOK)], hs)
    sent(wfull.at[pl.ds(0, 7)], ws)
    sent(attb.at[pl.ds(0, 7)], as_)
    sent(out.at[:, my_half], os_)


def per_device(latent, context, cond, cctx, shw, scw, gw, gain, wq, wk, wv, qg, kg, bias, outw):
    hbm = pl.BlockSpec(memory_space=pltpu.HBM)
    vm = pl.BlockSpec(memory_space=pltpu.VMEM)
    bf, f32 = jnp.bfloat16, jnp.float32
    dma = pltpu.SemaphoreType.DMA
    scratch = [
        pltpu.VMEM((2, 1, 16), f32),
        pltpu.VMEM((3, 16, F), bf),
        pltpu.VMEM((1, D), f32),
        pltpu.VMEM((2, 1, HD), f32),
        pltpu.SMEM((15, 2, 31), f32),
        pltpu.VMEM((5, F), f32),
        pltpu.VMEM((Y - 1, 5, F), f32),
        pltpu.VMEM((5, F), f32),
        pltpu.VMEM((Z - 1, 5, F), f32),
        pltpu.VMEM((TP, 5, F), f32),
        pltpu.VMEM((TP, 2, Z, 4, F), bf),
        pltpu.VMEM((128, D), f32),
        pltpu.VMEM((4, 128, 256), bf),
        pltpu.VMEM((TOK, D), f32),
        pltpu.VMEM((TOK, D), bf),
        pltpu.VMEM((128, D), bf),
        pltpu.VMEM((D, 384), bf),
        pltpu.VMEM((TP, 128, HALF), bf),
        pltpu.VMEM((TOK, D), bf),
        pltpu.VMEM((2, 14, COLS, 128), f32),
        pltpu.VMEM((3 * TOK, 256), bf),
        pltpu.VMEM((ROWS, 128, 128), bf),
        pltpu.VMEM((ROWS, 128, 512), f32),
        pltpu.VMEM((TP, TOK, 128), bf),
        pltpu.SemaphoreType.REGULAR,
        dma((5,)),
        dma((4,)),
    ]
    one = dma
    scratch += [one] * 6
    scratch += [dma((2,)), dma((2,)), one, dma((4,)), one, one, dma((2,))]
    scratch += [one, one, one, dma((4,))]
    scratch += [one, dma((6,)), dma((2,)), one, one]
    return pl.pallas_call(
        kernel,
        out_shape=jax.ShapeDtypeStruct((TOK, D), bf),
        in_specs=[hbm] * 15,
        out_specs=vm,
        scratch_shapes=scratch,
        compiler_params=pltpu.CompilerParams(
            collective_id=0, has_side_effects=True, vmem_limit_bytes=40 * 1024 * 1024
        ),
        name="fused",
    )(
        *(
            pltpu.with_memory_space_constraint(a, pltpu.HBM)
            for a in (
                latent, context, cond.reshape(1, 16), cctx.reshape(1, 16), shw, scw, gw, gain.reshape(1, D),
                wq, wk, wv, qg.reshape(1, HD), kg.reshape(1, HD), bias.transpose(1, 0, 2), outw,
            )
        )
    )


def solution(mesh):
    placed = (
        P("sp", None), P("sp", None), P("sp"), P("sp"),
        P("sp", "tp"), P("sp", "tp"), P("sp", "tp"), P(),
        P(None, "tp"), P(None, "tp"), P(None, "tp"), P(), P(),
        P("tp", None, None), P("tp", None),
    )
    return jax.shard_map(
        per_device, mesh=mesh, in_specs=placed, out_specs=P("sp", None), check_vma=False
    )
```

```python
import jax
import jax.numpy as jnp
from jax import lax
from jax.experimental import pallas as pl
from jax.experimental.pallas import tpu as pltpu
from jax.sharding import PartitionSpec as P

MESH = pl.DeviceIdType.MESH
EPS = 1e-06
Z, Y, TP = 16, 8, 8
SP = Z * Y
D = 2048
F = D // TP
TOK = 256
COLS = 64
ROWS = 4
HD = 64
HALF = D // 2
NEG = float("-inf")


def rem(a, n):
    return lax.rem(a, jnp.int32(n))


def head_norm(p, gain2):
    lane = lax.broadcasted_iota(jnp.int32, p.shape, 1)
    left = lane < HD
    sq = p * p
    s0 = jnp.sum(jnp.where(left, sq, 0.0), axis=1, keepdims=True)
    s1 = jnp.sum(jnp.where(left, 0.0, sq), axis=1, keepdims=True)
    r0 = lax.rsqrt(s0 * (1.0 / HD) + EPS)
    r1 = lax.rsqrt(s1 * (1.0 / HD) + EPS)
    return p * jnp.where(left, r0, r1) * gain2


def kernel(
    latent, context, cond_h, cctx_h, shw_h, scw_h, gw_h, gain_h, wq, wk, wv, qg_h, kg_h, bias_h, outw,
    out,
    cc, modw, gain, qkg, bias,
    part, mody, zpart, modz, modf,
    cbuf, cf, ckv,
    xn, hid, chid,
    wall, wfull, latv,
    tbl, kvp, q2, ew, attb,
    relay, small_sem, loc_sem,
    ys, yr, zs, zr, ts, tr,
    czs, czr, cts, ctr, cpr, cys, cyr,
    hs, hr, ws, wr,
    as_, ar, apr, os_, or_,
):
    sp = lax.axis_index("sp")
    tp = lax.axis_index("tp")
    y = rem(sp, Y)
    z = lax.div(sp, jnp.int32(Y))
    c = rem(tp, 2)
    odd = rem(y, 2)
    mate = y + 1 - 2 * odd
    side = 2 * odd - 1
    pair = lax.div(y, jnp.int32(2))
    partner = tp + 1 - 2 * c
    up = rem(sp + 1, SP)
    down = rem(sp + SP - 1, SP)
    right = rem(tp + 2, TP)
    left = rem(tp + TP - 2, TP)
    far = rem(tp + 4, TP)

    def at(s, t):
        return {"sp": s, "tp": t}

    def y_peer(k):
        return at(z * Y + rem(y + k, Y), tp)

    def z_peer(k):
        return at(rem(z + k, Z) * Y + y, tp)

    def m_peer(k):
        return at(rem(z + k, Z) * Y + mate, tp)

    def t_peer(k):
        return at(sp, rem(tp + k, TP))

    def remote(src, dst, s, r, dev):
        return pltpu.make_async_remote_copy(
            src_ref=src, dst_ref=dst, send_sem=s, recv_sem=r, device_id=dev, device_id_type=MESH
        )

    def send(src, dst, s, r, dev):
        remote(src, dst, s, r, dev).start()

    def arrived(ref, r):
        remote(ref, ref, r, r, at(sp, partner)).wait_recv()

    def sent(ref, s):
        remote(ref, ref, s, s, at(sp, partner)).wait_send()

    barrier = pltpu.get_barrier_semaphore()
    near = (4, 12, 3, 13, 2, 14, 1, 15)
    beyond = (8, 7, 9, 6, 10, 5, 11)
    y_order = (4, 3, 5, 2, 6, 1, 7)
    peers = [y_peer(k) for k in y_order]
    peers += [z_peer(k) for k in near] + [m_peer(k) for k in near + (0,)]
    peers += [t_peer(k) for k in range(1, TP)]
    peers += [at(up, tp), at(down, tp)]
    for p in peers:
        pl.semaphore_signal(barrier, inc=1, device_id=p, device_id_type=MESH)

    small = (
        (cond_h, cc.at[0], 0), (cctx_h, cc.at[1], 0),
        (shw_h, modw.at[0], 1), (scw_h, modw.at[1], 1), (gw_h, modw.at[2], 1),
        (bias_h, bias, 2), (gain_h, gain, 3), (qg_h, qkg.at[0], 4), (kg_h, qkg.at[1], 4),
    )
    for src, dst, n in small:
        pltpu.make_async_copy(src, dst, small_sem.at[n]).start()
    ctx_col = pl.multiple_of(tp * F, F)
    my_half = pl.ds(pl.multiple_of(c * HALF, HALF), HALF)
    its_half = pl.ds(pl.multiple_of((1 - c) * HALF, HALF), HALF)
    own_ctx = cbuf.at[tp, odd, z]
    own_c = pltpu.make_async_copy(context.at[:, pl.ds(ctx_col, F)], own_ctx, loc_sem.at[0])
    own_l = pltpu.make_async_copy(latent, latv, loc_sem.at[1])
    own_w = pltpu.make_async_copy(outw.at[:, my_half], wfull.at[tp], loc_sem.at[2])
    own_c.start()
    own_l.start()
    own_w.start()
    for n, src in enumerate((wk, wv, wq)):
        pltpu.make_async_copy(src, wall.at[:, pl.ds(n * 128, 128)], loc_sem.at[3]).start()

    pl.semaphore_wait(barrier, len(peers))
    for k in (4, Z - 4):
        pl.semaphore_signal(relay, inc=1, device_id=z_peer(k), device_id_type=MESH)

    pltpu.make_async_copy(cc, cc, small_sem.at[0]).wait()
    pltpu.make_async_copy(modw, modw, small_sem.at[1]).wait()
    row8 = lax.broadcasted_iota(jnp.int32, (8, 16), 0)
    pre = jnp.where(row8 == 0, jnp.broadcast_to(cc[0], (8, 16)), jnp.broadcast_to(cc[1], (8, 16)))
    act = (pre / (1.0 + jnp.exp(-pre))).astype(jnp.bfloat16)
    p_sh = jnp.dot(act, modw[0], preferred_element_type=jnp.float32)
    p_sc = jnp.dot(act, modw[1], preferred_element_type=jnp.float32)
    p_g = jnp.dot(act, modw[2], preferred_element_type=jnp.float32)
    part[0:2, :] = p_sh[0:2]
    part[2:4, :] = p_sc[0:2]
    part[4:5, :] = p_g[0:1]

    def other(t):
        return t + 1 - 2 * c

    for k in y_order:
        send(part, mody.at[k - 1], ys, yr, y_peer(k))
    own_c.wait()
    for k in near:
        send(own_ctx, own_ctx, czs.at[0], czr.at[0], z_peer(k))
        send(own_ctx, own_ctx, czs.at[1], czr.at[1], m_peer(k))
    send(own_ctx, own_ctx, czs.at[1], czr.at[1], m_peer(0))
    send(outw.at[:, its_half], wfull.at[tp], ws, wr.at[0], at(sp, partner))
    send(outw.at[:, my_half], wfull.at[tp], ws, wr.at[1], at(sp, right))
    send(outw.at[:, my_half], wfull.at[tp], ws, wr.at[1], at(sp, left))
    send(outw.at[:, its_half], wfull.at[tp], ws, wr.at[2], at(sp, other(right)))
    send(outw.at[:, its_half], wfull.at[tp], ws, wr.at[2], at(sp, other(left)))

    pl.semaphore_wait(relay, 2)
    for k in beyond:
        send(own_ctx, own_ctx, czs.at[0], czr.at[0], z_peer(k))
        send(own_ctx, own_ctx, czs.at[1], czr.at[1], m_peer(k))

    arrived(mody, yr)
    acc = part[...]
    for k in range(1, Y):
        acc = acc + mody[k - 1]
    zpart[...] = acc
    for k in beyond + near:
        send(zpart, modz.at[k - 1], zs, zr, z_peer(k))

    tq = lax.broadcasted_iota(jnp.int32, (COLS, 128), 0)
    tl = lax.broadcasted_iota(jnp.int32, (COLS, 128), 1)
    tk = jnp.where(tl < COLS, tl, tl - COLS)
    diff = tk - tq + 15
    c0 = jnp.clip(tq - 8, 0, 48)
    is_open = (tk >= c0) & (tk < c0 + 16)
    first = lax.broadcasted_iota(jnp.int32, (1, 128), 1) < COLS

    def table_step(n, carry):
        h = lax.div(n, jnp.int32(14))
        a = rem(n, 14)
        val = jnp.full((COLS, 128), NEG, jnp.float32)
        for dd in range(31):
            v = jnp.where(first, bias[a, h, dd], bias[a + 1, h, dd])
            val = jnp.where(diff == dd, jnp.broadcast_to(v, (COLS, 128)), val)
        tbl[h, a] = jnp.where(is_open, val, NEG)
        return carry

    pltpu.make_async_copy(bias_h, bias, small_sem.at[2]).wait()
    lax.fori_loop(0, 28, table_step, 0)
    pltpu.make_async_copy(gain_h, gain, small_sem.at[3]).wait()

    def normed(load, store, rows, chunk):
        def step(n, carry):
            r = pl.ds(pl.multiple_of(n * chunk, chunk), chunk)
            v = load(r).astype(jnp.float32)
            ms = jnp.mean(v * v, axis=-1, keepdims=True)
            store(r, v * lax.rsqrt(ms + EPS) * gain[...])
            return carry

        lax.fori_loop(0, rows // chunk, step, 0)

    own_l.wait()

    def store_own(r, v):
        xn[r, :] = v

    normed(lambda r: latv[r, :], store_own, TOK, 16)

    arrived(cbuf.at[0, 0, pl.ds(0, Z - 1)], czr.at[0])
    arrived(cbuf.at[0, 0], czr.at[1])
    hops = ((far, 0), (right, 1), (left, 2), (partner, 3))
    for t, n in hops:
        send(cbuf.at[tp], cbuf.at[tp], cts, ctr.at[n], at(sp, t))

    arrived(modz, zr)
    acc = zpart[...]
    for k in range(1, Z):
        acc = acc + modz[k - 1]
    modf[tp] = acc
    for k in (4, 3, 5, 2, 6, 1, 7):
        send(modf.at[tp], modf.at[tp], ts, tr, t_peer(k))

    for n, frm in ((1, left), (2, right), (0, far)):
        arrived(cbuf.at[frm], ctr.at[n])
        send(cbuf.at[frm], cbuf.at[frm], cts, cpr, at(sp, partner))

    arrived(cbuf.at[partner], ctr.at[3])
    arrived(cbuf.at[pl.ds(0, 3)], cpr)

    for j in range(2 * Z):
        for g in range(TP):
            cf[4 * j : 4 * j + 4, g * F : (g + 1) * F] = cbuf[g, j % 2, j // 2].astype(jnp.float32)

    def store_ctx(r, v):
        cf[r, :] = v

    normed(lambda r: cf[r, :], store_ctx, 128, 16)

    pltpu.make_async_copy(wall, wall, loc_sem.at[3]).wait()
    pltpu.make_async_copy(qkg, qkg, small_sem.at[4]).wait()
    arrived(modf.at[pl.ds(0, TP - 1)], tr)
    lane = lax.broadcasted_iota(jnp.int32, (1, 128), 1)
    qg2 = jnp.concatenate([qkg[0], qkg[0]], axis=1)
    kg2 = jnp.concatenate([qkg[1], qkg[1]], axis=1)

    for g in range(TP):
        gs = slice(g * F, (g + 1) * F)
        chid[:, gs] = (cf[:, gs] * (1.0 + modf[g, 3:4, :]) + modf[g, 1:2, :]).astype(jnp.bfloat16)
    kv = jnp.dot(chid[...], wall[:, 0:256], preferred_element_type=jnp.float32)
    ckv[pair, :, 0:128] = head_norm(kv[:, 0:128], kg2).astype(jnp.bfloat16)
    ckv[pair, :, 128:256] = kv[:, 128:256].astype(jnp.bfloat16)
    zh = rem(z, 2)
    zmate = at((z + 1 - 2 * zh) * Y + y, tp)
    tok_half = pl.ds(pl.multiple_of(zh * 64, 64), 64)
    own_pair = ckv.at[pair, tok_half]
    for k in (3, 2, 1):
        send(own_pair, own_pair, cys, cyr.at[k - 1], at(z * Y + rem(y + k * side + Y, Y), tp))

    for n in range(2):
        r = pl.ds(n * 128, 128)
        for g in range(TP):
            gs = slice(g * F, (g + 1) * F)
            hid[r, gs] = (xn[r, gs] * (1.0 + modf[g, 2:3, :]) + modf[g, 0:1, :]).astype(jnp.bfloat16)
        h = hid[r, :]
        kv = jnp.dot(h, wall[:, 0:256], preferred_element_type=jnp.float32)
        kr = pl.ds(TOK + n * 128, 128)
        kvp[kr, 0:128] = head_norm(kv[:, 0:128], kg2).astype(jnp.bfloat16)
        kvp[kr, 128:256] = kv[:, 128:256].astype(jnp.bfloat16)
    own_rows = kvp.at[pl.ds(TOK, TOK)]
    send(own_rows, kvp.at[pl.ds(0, TOK)], hs, hr, at(up, tp))
    send(own_rows, kvp.at[pl.ds(2 * TOK, TOK)], hs, hr, at(down, tp))

    for n in range(2):
        r = pl.ds(n * 128, 128)
        q = jnp.dot(hid[r, :], wall[:, 256:384], preferred_element_type=jnp.float32)
        q = (head_norm(q, qg2) * (HD**-0.5)).astype(jnp.bfloat16)
        zero = jnp.zeros_like(q)
        lf = jnp.broadcast_to(lane < HD, q.shape)
        q0 = jnp.where(lf, q, zero)
        q1 = jnp.where(lf, zero, q)
        for i in range(2):
            q2[2 * n + i, 0:64, :] = q0[i * 64 : (i + 1) * 64]
            q2[2 * n + i, 64:128, :] = q1[i * 64 : (i + 1) * 64]

    lo, hi = pl.ds(0, 64), pl.ds(64, 64)
    arrived(wfull.at[pl.ds(0, 2)], wr.at[1])
    arrived(wfull.at[pl.ds(0, 2)], wr.at[2])
    for f in (left, other(left)):
        send(wfull.at[f, lo], wfull.at[f, lo], ws, wr.at[3], at(sp, right))
    for f in (right, other(right)):
        send(wfull.at[f, hi], wfull.at[f, hi], ws, wr.at[3], at(sp, left))

    for k, p in ((1, pair + side), (2, pair - side), (3, pair + 2)):
        got = ckv.at[rem(p + 4, 4), tok_half]
        arrived(got, cyr.at[k - 1])
        send(got, got, cys, cyr.at[3], zmate)

    arrived(kvp.at[pl.ds(0, 2 * TOK)], hr)

    nt = (((1,), (1,)), ((), ()))
    at_first = sp == 0
    at_last = sp == SP - 1
    m_w, l_w, band = [], [], []
    for i in range(ROWS):
        start = jnp.where(at_first, 4, jnp.where(at_last, 0, i))
        off = jnp.where(at_first, 7 - i, 3 + jnp.where(at_last, -i, 0))
        rows = pl.ds(pl.multiple_of(start * COLS, COLS), 8 * COLS)
        band.append(rows)
        s = lax.dot_general(q2[i], kvp[rows, 0:128], nt, preferred_element_type=jnp.float32)
        tiles = []
        for p in range(4):
            t = jnp.concatenate([tbl[0, off + 2 * p], tbl[1, off + 2 * p]], axis=0)
            tiles.append(s[:, p * 128 : (p + 1) * 128] + t)
        s = jnp.concatenate(tiles, axis=1)
        m = jnp.max(s, axis=1, keepdims=True)
        e = jnp.exp(s - m)
        ew[i] = e
        m_w.append(m)
        l_w.append(jnp.sum(e, axis=1, keepdims=True))

    arrived(ckv.at[pl.ds(0, 3), pl.ds(0, 64)], cyr.at[3])

    ck = ckv[:, :, 0:128].reshape(512, 128)
    cv = ckv[:, :, 128:256].reshape(512, 128)
    for i in range(ROWS):
        s = lax.dot_general(q2[i], ck, nt, preferred_element_type=jnp.float32)
        m = jnp.maximum(m_w[i], jnp.max(s, axis=1, keepdims=True))
        ec = jnp.exp(s - m)
        fw = jnp.exp(m_w[i] - m)
        inv = 1.0 / (l_w[i] * fw + jnp.sum(ec, axis=1, keepdims=True))
        w_win = (ew[i] * (fw * inv)).astype(jnp.bfloat16)
        w_ctx = (ec * inv).astype(jnp.bfloat16)
        o = jnp.dot(w_win, kvp[band[i], 128:256], preferred_element_type=jnp.float32) + jnp.dot(
            w_ctx, cv, preferred_element_type=jnp.float32
        )
        o = jnp.where(jnp.broadcast_to(lane < HD, (64, 128)), o[0:64], o[64:128])
        attb[tp, i * COLS : (i + 1) * COLS, :] = o.astype(jnp.bfloat16)
        if i % 2 == 1:
            hh = i // 2
            block = attb.at[tp, pl.ds(hh * 128, 128)]
            for t, n in hops:
                send(block, block, as_, apr.at[hh] if n == 3 else ar.at[hh * 3 + n], at(sp, t))

    for hh in range(2):
        rr = pl.ds(hh * 128, 128)
        for n, frm in ((1, left), (2, right), (0, far)):
            block = attb.at[frm, rr]
            arrived(block, ar.at[hh * 3 + n])
            send(block, block, as_, apr.at[hh], at(sp, partner))

    arrived(wfull.at[partner], wr.at[0])
    own_w.wait()
    arrived(wfull.at[pl.ds(0, 2)], wr.at[3])

    for hh in range(2):
        rr = pl.ds(hh * 128, 128)
        arrived(attb.at[pl.ds(0, 2)], apr.at[hh])
        for n in range(HALF // F):
            cols = pl.ds(pl.multiple_of(c * HALF + n * F, F), F)
            acc = jnp.zeros((128, F), jnp.float32)
            for g in range(TP):
                t = jnp.dot(attb[g, rr, :], wfull[g, :, n * F : (n + 1) * F], preferred_element_type=jnp.float32)
                acc = acc + t.astype(jnp.bfloat16).astype(jnp.float32)
            res = latv[rr, cols].astype(jnp.float32) + modf[c * (HALF // F) + n, 4:5, :] * acc
            out[rr, cols] = res.astype(jnp.bfloat16)
            send(out.at[rr, cols], out.at[rr, cols], os_, or_, at(sp, partner))
    arrived(out.at[:, its_half], or_)

    sent(mody, ys)
    sent(modz, zs)
    sent(modf.at[pl.ds(0, TP - 1)], ts)
    sent(cbuf.at[0, 0, pl.ds(0, Z - 1)], czs.at[0])
    sent(cbuf.at[0, 0], czs.at[1])
    sent(cbuf.at[pl.ds(0, 7)], cts)
    sent(ckv.at[pl.ds(0, 3)], cys)
    sent(kvp.at[pl.ds(0, 2 * TOK)], hs)
    sent(wfull.at[pl.ds(0, 7)], ws)
    sent(attb.at[pl.ds(0, 7)], as_)
    sent(out.at[:, my_half], os_)


def per_device(latent, context, cond, cctx, shw, scw, gw, gain, wq, wk, wv, qg, kg, bias, outw):
    hbm = pl.BlockSpec(memory_space=pltpu.HBM)
    vm = pl.BlockSpec(memory_space=pltpu.VMEM)
    bf, f32 = jnp.bfloat16, jnp.float32
    dma = pltpu.SemaphoreType.DMA
    scratch = [
        pltpu.VMEM((2, 1, 16), f32),
        pltpu.VMEM((3, 16, F), bf),
        pltpu.VMEM((1, D), f32),
        pltpu.VMEM((2, 1, HD), f32),
        pltpu.SMEM((15, 2, 31), f32),
        pltpu.VMEM((5, F), f32),
        pltpu.VMEM((Y - 1, 5, F), f32),
        pltpu.VMEM((5, F), f32),
        pltpu.VMEM((Z - 1, 5, F), f32),
        pltpu.VMEM((TP, 5, F), f32),
        pltpu.VMEM((TP, 2, Z, 4, F), bf),
        pltpu.VMEM((128, D), f32),
        pltpu.VMEM((4, 128, 256), bf),
        pltpu.VMEM((TOK, D), f32),
        pltpu.VMEM((TOK, D), bf),
        pltpu.VMEM((128, D), bf),
        pltpu.VMEM((D, 384), bf),
        pltpu.VMEM((TP, 128, HALF), bf),
        pltpu.VMEM((TOK, D), bf),
        pltpu.VMEM((2, 14, COLS, 128), f32),
        pltpu.VMEM((3 * TOK, 256), bf),
        pltpu.VMEM((ROWS, 128, 128), bf),
        pltpu.VMEM((ROWS, 128, 512), f32),
        pltpu.VMEM((TP, TOK, 128), bf),
        pltpu.SemaphoreType.REGULAR,
        dma((5,)),
        dma((4,)),
    ]
    one = dma
    scratch += [one] * 6
    scratch += [dma((2,)), dma((2,)), one, dma((4,)), one, one, dma((4,))]
    scratch += [one, one, one, dma((4,))]
    scratch += [one, dma((6,)), dma((2,)), one, one]
    return pl.pallas_call(
        kernel,
        out_shape=jax.ShapeDtypeStruct((TOK, D), bf),
        in_specs=[hbm] * 15,
        out_specs=vm,
        scratch_shapes=scratch,
        compiler_params=pltpu.CompilerParams(
            collective_id=0, has_side_effects=True, vmem_limit_bytes=40 * 1024 * 1024
        ),
        name="fused",
    )(
        *(
            pltpu.with_memory_space_constraint(a, pltpu.HBM)
            for a in (
                latent, context, cond.reshape(1, 16), cctx.reshape(1, 16), shw, scw, gw, gain.reshape(1, D),
                wq, wk, wv, qg.reshape(1, HD), kg.reshape(1, HD), bias.transpose(1, 0, 2), outw,
            )
        )
    )


def solution(mesh):
    placed = (
        P("sp", None), P("sp", None), P("sp"), P("sp"),
        P("sp", "tp"), P("sp", "tp"), P("sp", "tp"), P(),
        P(None, "tp"), P(None, "tp"), P(None, "tp"), P(), P(),
        P("tp", None, None), P("tp", None),
    )
    return jax.shard_map(
        per_device, mesh=mesh, in_specs=placed, out_specs=P("sp", None), check_vma=False
    )
```

```python
import jax
import jax.numpy as jnp
from jax import lax
from jax.experimental import pallas as pl
from jax.experimental.pallas import tpu as pltpu
from jax.sharding import PartitionSpec as P

MESH = pl.DeviceIdType.MESH
EPS = 1e-06
Z, Y, TP = 16, 8, 8
SP = Z * Y
D = 2048
F = D // TP
TOK = 256
COLS = 64
ROWS = 4
HD = 64
HALF = D // 2
NEG = float("-inf")


def rem(a, n):
    return lax.rem(a, jnp.int32(n))


def head_norm(p, gain2):
    lane = lax.broadcasted_iota(jnp.int32, p.shape, 1)
    left = lane < HD
    sq = p * p
    s0 = jnp.sum(jnp.where(left, sq, 0.0), axis=1, keepdims=True)
    s1 = jnp.sum(jnp.where(left, 0.0, sq), axis=1, keepdims=True)
    r0 = lax.rsqrt(s0 * (1.0 / HD) + EPS)
    r1 = lax.rsqrt(s1 * (1.0 / HD) + EPS)
    return p * jnp.where(left, r0, r1) * gain2


def kernel(
    latent, context, cond_h, cctx_h, shw_h, scw_h, gw_h, gain_h, wq, wk, wv, qg_h, kg_h, bias_h, outw,
    out,
    cc, modw, gain, qkg, bias,
    part, mody, zpart, modz, modf,
    cbuf, cf, ckv,
    xn, hid, chid,
    wall, wfull, latv,
    tbl, kvp, q2, ew, attb,
    relay, small_sem, loc_sem,
    ys, yr, zs, zr, ts, tr,
    czs, czr, cts, ctr, cpr, cys, cyr,
    hs, hr, ws, wr,
    as_, ar, apr, os_, or_,
):
    sp = lax.axis_index("sp")
    tp = lax.axis_index("tp")
    y = rem(sp, Y)
    z = lax.div(sp, jnp.int32(Y))
    c = rem(tp, 2)
    odd = rem(y + 1, 2)
    mate = rem(y + Y + 1 - 2 * odd, Y)
    side = 2 * odd - 1
    pair = rem(lax.div(y + 1, jnp.int32(2)), 4)
    partner = tp + 1 - 2 * c
    up = rem(sp + 1, SP)
    down = rem(sp + SP - 1, SP)
    right = rem(tp + 2, TP)
    left = rem(tp + TP - 2, TP)
    far = rem(tp + 4, TP)

    def at(s, t):
        return {"sp": s, "tp": t}

    def y_peer(k):
        return at(z * Y + rem(y + k, Y), tp)

    def z_peer(k):
        return at(rem(z + k, Z) * Y + y, tp)

    def m_peer(k):
        return at(rem(z + k, Z) * Y + mate, tp)

    def t_peer(k):
        return at(sp, rem(tp + k, TP))

    def remote(src, dst, s, r, dev):
        return pltpu.make_async_remote_copy(
            src_ref=src, dst_ref=dst, send_sem=s, recv_sem=r, device_id=dev, device_id_type=MESH
        )

    def send(src, dst, s, r, dev):
        remote(src, dst, s, r, dev).start()

    def arrived(ref, r):
        remote(ref, ref, r, r, at(sp, partner)).wait_recv()

    def sent(ref, s):
        remote(ref, ref, s, s, at(sp, partner)).wait_send()

    barrier = pltpu.get_barrier_semaphore()
    near = (4, 12, 3, 13, 2, 14, 1, 15)
    beyond = (8, 7, 9, 6, 10, 5, 11)
    y_order = (4, 3, 5, 2, 6, 1, 7)
    peers = [y_peer(k) for k in y_order]
    peers += [z_peer(k) for k in near] + [m_peer(k) for k in near + (0,)]
    peers += [t_peer(k) for k in range(1, TP)]
    peers += [at(up, tp), at(down, tp)]
    for p in peers:
        pl.semaphore_signal(barrier, inc=1, device_id=p, device_id_type=MESH)

    small = (
        (cond_h, cc.at[0], 0), (cctx_h, cc.at[1], 0),
        (shw_h, modw.at[0], 1), (scw_h, modw.at[1], 1), (gw_h, modw.at[2], 1),
        (bias_h, bias, 2), (gain_h, gain, 3), (qg_h, qkg.at[0], 4), (kg_h, qkg.at[1], 4),
    )
    for src, dst, n in small:
        pltpu.make_async_copy(src, dst, small_sem.at[n]).start()
    ctx_col = pl.multiple_of(tp * F, F)
    my_half = pl.ds(pl.multiple_of(c * HALF, HALF), HALF)
    its_half = pl.ds(pl.multiple_of((1 - c) * HALF, HALF), HALF)
    own_ctx = cbuf.at[tp, odd, z]
    own_c = pltpu.make_async_copy(context.at[:, pl.ds(ctx_col, F)], own_ctx, loc_sem.at[0])
    own_l = pltpu.make_async_copy(latent, latv, loc_sem.at[1])
    own_w = pltpu.make_async_copy(outw.at[:, my_half], wfull.at[tp], loc_sem.at[2])
    own_c.start()
    own_l.start()
    own_w.start()
    for n, src in enumerate((wk, wv, wq)):
        pltpu.make_async_copy(src, wall.at[:, pl.ds(n * 128, 128)], loc_sem.at[3]).start()

    pl.semaphore_wait(barrier, len(peers))
    for k in (4, Z - 4):
        pl.semaphore_signal(relay, inc=1, device_id=z_peer(k), device_id_type=MESH)

    pltpu.make_async_copy(cc, cc, small_sem.at[0]).wait()
    pltpu.make_async_copy(modw, modw, small_sem.at[1]).wait()
    row8 = lax.broadcasted_iota(jnp.int32, (8, 16), 0)
    pre = jnp.where(row8 == 0, jnp.broadcast_to(cc[0], (8, 16)), jnp.broadcast_to(cc[1], (8, 16)))
    act = (pre / (1.0 + jnp.exp(-pre))).astype(jnp.bfloat16)
    p_sh = jnp.dot(act, modw[0], preferred_element_type=jnp.float32)
    p_sc = jnp.dot(act, modw[1], preferred_element_type=jnp.float32)
    p_g = jnp.dot(act, modw[2], preferred_element_type=jnp.float32)
    part[0:2, :] = p_sh[0:2]
    part[2:4, :] = p_sc[0:2]
    part[4:5, :] = p_g[0:1]

    def other(t):
        return t + 1 - 2 * c

    for k in y_order:
        send(part, mody.at[k - 1], ys, yr, y_peer(k))
    own_c.wait()
    for k in near:
        send(own_ctx, own_ctx, czs.at[0], czr.at[0], z_peer(k))
        send(own_ctx, own_ctx, czs.at[1], czr.at[1], m_peer(k))
    send(own_ctx, own_ctx, czs.at[1], czr.at[1], m_peer(0))
    send(outw.at[:, its_half], wfull.at[tp], ws, wr.at[0], at(sp, partner))
    send(outw.at[:, my_half], wfull.at[tp], ws, wr.at[1], at(sp, right))
    send(outw.at[:, my_half], wfull.at[tp], ws, wr.at[1], at(sp, left))
    send(outw.at[:, its_half], wfull.at[tp], ws, wr.at[2], at(sp, other(right)))
    send(outw.at[:, its_half], wfull.at[tp], ws, wr.at[2], at(sp, other(left)))

    pl.semaphore_wait(relay, 2)
    for k in beyond:
        send(own_ctx, own_ctx, czs.at[0], czr.at[0], z_peer(k))
        send(own_ctx, own_ctx, czs.at[1], czr.at[1], m_peer(k))

    arrived(mody, yr)
    acc = part[...]
    for k in range(1, Y):
        acc = acc + mody[k - 1]
    zpart[...] = acc
    for k in beyond + near:
        send(zpart, modz.at[k - 1], zs, zr, z_peer(k))

    tq = lax.broadcasted_iota(jnp.int32, (COLS, 128), 0)
    tl = lax.broadcasted_iota(jnp.int32, (COLS, 128), 1)
    tk = jnp.where(tl < COLS, tl, tl - COLS)
    diff = tk - tq + 15
    c0 = jnp.clip(tq - 8, 0, 48)
    is_open = (tk >= c0) & (tk < c0 + 16)
    first = lax.broadcasted_iota(jnp.int32, (1, 128), 1) < COLS

    def table_step(n, carry):
        h = lax.div(n, jnp.int32(14))
        a = rem(n, 14)
        val = jnp.full((COLS, 128), NEG, jnp.float32)
        for dd in range(31):
            v = jnp.where(first, bias[a, h, dd], bias[a + 1, h, dd])
            val = jnp.where(diff == dd, jnp.broadcast_to(v, (COLS, 128)), val)
        tbl[h, a] = jnp.where(is_open, val, NEG)
        return carry

    pltpu.make_async_copy(bias_h, bias, small_sem.at[2]).wait()
    lax.fori_loop(0, 28, table_step, 0)
    pltpu.make_async_copy(gain_h, gain, small_sem.at[3]).wait()

    def normed(load, store, rows, chunk):
        def step(n, carry):
            r = pl.ds(pl.multiple_of(n * chunk, chunk), chunk)
            v = load(r).astype(jnp.float32)
            ms = jnp.mean(v * v, axis=-1, keepdims=True)
            store(r, v * lax.rsqrt(ms + EPS) * gain[...])
            return carry

        lax.fori_loop(0, rows // chunk, step, 0)

    own_l.wait()

    def store_own(r, v):
        xn[r, :] = v

    normed(lambda r: latv[r, :], store_own, TOK, 16)

    arrived(cbuf.at[0, 0, pl.ds(0, Z - 1)], czr.at[0])
    arrived(cbuf.at[0, 0], czr.at[1])
    hops = ((far, 0), (right, 1), (left, 2), (partner, 3))
    for t, n in hops:
        send(cbuf.at[tp], cbuf.at[tp], cts, ctr.at[n], at(sp, t))

    arrived(modz, zr)
    acc = zpart[...]
    for k in range(1, Z):
        acc = acc + modz[k - 1]
    modf[tp] = acc
    for k in (4, 3, 5, 2, 6, 1, 7):
        send(modf.at[tp], modf.at[tp], ts, tr, t_peer(k))

    for n, frm in ((1, left), (2, right), (0, far)):
        arrived(cbuf.at[frm], ctr.at[n])
        send(cbuf.at[frm], cbuf.at[frm], cts, cpr, at(sp, partner))

    arrived(cbuf.at[partner], ctr.at[3])
    arrived(cbuf.at[pl.ds(0, 3)], cpr)

    for j in range(2 * Z):
        for g in range(TP):
            cf[4 * j : 4 * j + 4, g * F : (g + 1) * F] = cbuf[g, j % 2, j // 2].astype(jnp.float32)

    def store_ctx(r, v):
        cf[r, :] = v

    normed(lambda r: cf[r, :], store_ctx, 128, 16)

    pltpu.make_async_copy(wall, wall, loc_sem.at[3]).wait()
    pltpu.make_async_copy(qkg, qkg, small_sem.at[4]).wait()
    arrived(modf.at[pl.ds(0, TP - 1)], tr)
    lane = lax.broadcasted_iota(jnp.int32, (1, 128), 1)
    qg2 = jnp.concatenate([qkg[0], qkg[0]], axis=1)
    kg2 = jnp.concatenate([qkg[1], qkg[1]], axis=1)

    for g in range(TP):
        gs = slice(g * F, (g + 1) * F)
        chid[:, gs] = (cf[:, gs] * (1.0 + modf[g, 3:4, :]) + modf[g, 1:2, :]).astype(jnp.bfloat16)
    kv = jnp.dot(chid[...], wall[:, 0:256], preferred_element_type=jnp.float32)
    ckv[pair, :, 0:128] = head_norm(kv[:, 0:128], kg2).astype(jnp.bfloat16)
    ckv[pair, :, 128:256] = kv[:, 128:256].astype(jnp.bfloat16)
    zh = rem(z, 2)
    zmate = at((z + 1 - 2 * zh) * Y + y, tp)
    tok_half = pl.ds(pl.multiple_of(zh * 64, 64), 64)
    own_pair = ckv.at[pair, tok_half]
    for k in (3, 2, 1):
        send(own_pair, own_pair, cys, cyr.at[k - 1], at(z * Y + rem(y + k * side + Y, Y), tp))

    for n in range(2):
        r = pl.ds(n * 128, 128)
        for g in range(TP):
            gs = slice(g * F, (g + 1) * F)
            hid[r, gs] = (xn[r, gs] * (1.0 + modf[g, 2:3, :]) + modf[g, 0:1, :]).astype(jnp.bfloat16)
        h = hid[r, :]
        kv = jnp.dot(h, wall[:, 0:256], preferred_element_type=jnp.float32)
        kr = pl.ds(TOK + n * 128, 128)
        kvp[kr, 0:128] = head_norm(kv[:, 0:128], kg2).astype(jnp.bfloat16)
        kvp[kr, 128:256] = kv[:, 128:256].astype(jnp.bfloat16)
    own_rows = kvp.at[pl.ds(TOK, TOK)]
    send(own_rows, kvp.at[pl.ds(0, TOK)], hs, hr, at(up, tp))
    send(own_rows, kvp.at[pl.ds(2 * TOK, TOK)], hs, hr, at(down, tp))

    for n in range(2):
        r = pl.ds(n * 128, 128)
        q = jnp.dot(hid[r, :], wall[:, 256:384], preferred_element_type=jnp.float32)
        q = (head_norm(q, qg2) * (HD**-0.5)).astype(jnp.bfloat16)
        zero = jnp.zeros_like(q)
        lf = jnp.broadcast_to(lane < HD, q.shape)
        q0 = jnp.where(lf, q, zero)
        q1 = jnp.where(lf, zero, q)
        for i in range(2):
            q2[2 * n + i, 0:64, :] = q0[i * 64 : (i + 1) * 64]
            q2[2 * n + i, 64:128, :] = q1[i * 64 : (i + 1) * 64]

    lo, hi = pl.ds(0, 64), pl.ds(64, 64)
    arrived(wfull.at[pl.ds(0, 2)], wr.at[1])
    arrived(wfull.at[pl.ds(0, 2)], wr.at[2])
    for f in (left, other(left)):
        send(wfull.at[f, lo], wfull.at[f, lo], ws, wr.at[3], at(sp, right))
    for f in (right, other(right)):
        send(wfull.at[f, hi], wfull.at[f, hi], ws, wr.at[3], at(sp, left))

    for k, p in ((1, pair + side), (2, pair - side), (3, pair + 2)):
        got = ckv.at[rem(p + 4, 4), tok_half]
        arrived(got, cyr.at[k - 1])
        send(got, got, cys, cyr.at[3], zmate)

    arrived(kvp.at[pl.ds(0, 2 * TOK)], hr)

    nt = (((1,), (1,)), ((), ()))
    at_first = sp == 0
    at_last = sp == SP - 1
    m_w, l_w, band = [], [], []
    for i in range(ROWS):
        start = jnp.where(at_first, 4, jnp.where(at_last, 0, i))
        off = jnp.where(at_first, 7 - i, 3 + jnp.where(at_last, -i, 0))
        rows = pl.ds(pl.multiple_of(start * COLS, COLS), 8 * COLS)
        band.append(rows)
        s = lax.dot_general(q2[i], kvp[rows, 0:128], nt, preferred_element_type=jnp.float32)
        tiles = []
        for p in range(4):
            t = jnp.concatenate([tbl[0, off + 2 * p], tbl[1, off + 2 * p]], axis=0)
            tiles.append(s[:, p * 128 : (p + 1) * 128] + t)
        s = jnp.concatenate(tiles, axis=1)
        m = jnp.max(s, axis=1, keepdims=True)
        e = jnp.exp(s - m)
        ew[i] = e
        m_w.append(m)
        l_w.append(jnp.sum(e, axis=1, keepdims=True))

    arrived(ckv.at[pl.ds(0, 3), pl.ds(0, 64)], cyr.at[3])

    ck = ckv[:, :, 0:128].reshape(512, 128)
    cv = ckv[:, :, 128:256].reshape(512, 128)
    for i in range(ROWS):
        s = lax.dot_general(q2[i], ck, nt, preferred_element_type=jnp.float32)
        m = jnp.maximum(m_w[i], jnp.max(s, axis=1, keepdims=True))
        ec = jnp.exp(s - m)
        fw = jnp.exp(m_w[i] - m)
        inv = 1.0 / (l_w[i] * fw + jnp.sum(ec, axis=1, keepdims=True))
        w_win = (ew[i] * (fw * inv)).astype(jnp.bfloat16)
        w_ctx = (ec * inv).astype(jnp.bfloat16)
        o = jnp.dot(w_win, kvp[band[i], 128:256], preferred_element_type=jnp.float32) + jnp.dot(
            w_ctx, cv, preferred_element_type=jnp.float32
        )
        o = jnp.where(jnp.broadcast_to(lane < HD, (64, 128)), o[0:64], o[64:128])
        attb[tp, i * COLS : (i + 1) * COLS, :] = o.astype(jnp.bfloat16)
        if i % 2 == 1:
            hh = i // 2
            block = attb.at[tp, pl.ds(hh * 128, 128)]
            for t, n in hops:
                send(block, block, as_, apr.at[hh] if n == 3 else ar.at[hh * 3 + n], at(sp, t))

    for hh in range(2):
        rr = pl.ds(hh * 128, 128)
        for n, frm in ((1, left), (2, right), (0, far)):
            block = attb.at[frm, rr]
            arrived(block, ar.at[hh * 3 + n])
            send(block, block, as_, apr.at[hh], at(sp, partner))

    arrived(wfull.at[partner], wr.at[0])
    own_w.wait()
    arrived(wfull.at[pl.ds(0, 2)], wr.at[3])

    for hh in range(2):
        rr = pl.ds(hh * 128, 128)
        arrived(attb.at[pl.ds(0, 2)], apr.at[hh])
        for n in range(HALF // F):
            cols = pl.ds(pl.multiple_of(c * HALF + n * F, F), F)
            acc = jnp.zeros((128, F), jnp.float32)
            for g in range(TP):
                t = jnp.dot(attb[g, rr, :], wfull[g, :, n * F : (n + 1) * F], preferred_element_type=jnp.float32)
                acc = acc + t.astype(jnp.bfloat16).astype(jnp.float32)
            res = latv[rr, cols].astype(jnp.float32) + modf[c * (HALF // F) + n, 4:5, :] * acc
            out[rr, cols] = res.astype(jnp.bfloat16)
            send(out.at[rr, cols], out.at[rr, cols], os_, or_, at(sp, partner))
    arrived(out.at[:, its_half], or_)

    sent(mody, ys)
    sent(modz, zs)
    sent(modf.at[pl.ds(0, TP - 1)], ts)
    sent(cbuf.at[0, 0, pl.ds(0, Z - 1)], czs.at[0])
    sent(cbuf.at[0, 0], czs.at[1])
    sent(cbuf.at[pl.ds(0, 7)], cts)
    sent(ckv.at[pl.ds(0, 3)], cys)
    sent(kvp.at[pl.ds(0, 2 * TOK)], hs)
    sent(wfull.at[pl.ds(0, 7)], ws)
    sent(attb.at[pl.ds(0, 7)], as_)
    sent(out.at[:, my_half], os_)


def per_device(latent, context, cond, cctx, shw, scw, gw, gain, wq, wk, wv, qg, kg, bias, outw):
    hbm = pl.BlockSpec(memory_space=pltpu.HBM)
    vm = pl.BlockSpec(memory_space=pltpu.VMEM)
    bf, f32 = jnp.bfloat16, jnp.float32
    dma = pltpu.SemaphoreType.DMA
    scratch = [
        pltpu.VMEM((2, 1, 16), f32),
        pltpu.VMEM((3, 16, F), bf),
        pltpu.VMEM((1, D), f32),
        pltpu.VMEM((2, 1, HD), f32),
        pltpu.SMEM((15, 2, 31), f32),
        pltpu.VMEM((5, F), f32),
        pltpu.VMEM((Y - 1, 5, F), f32),
        pltpu.VMEM((5, F), f32),
        pltpu.VMEM((Z - 1, 5, F), f32),
        pltpu.VMEM((TP, 5, F), f32),
        pltpu.VMEM((TP, 2, Z, 4, F), bf),
        pltpu.VMEM((128, D), f32),
        pltpu.VMEM((4, 128, 256), bf),
        pltpu.VMEM((TOK, D), f32),
        pltpu.VMEM((TOK, D), bf),
        pltpu.VMEM((128, D), bf),
        pltpu.VMEM((D, 384), bf),
        pltpu.VMEM((TP, 128, HALF), bf),
        pltpu.VMEM((TOK, D), bf),
        pltpu.VMEM((2, 14, COLS, 128), f32),
        pltpu.VMEM((3 * TOK, 256), bf),
        pltpu.VMEM((ROWS, 128, 128), bf),
        pltpu.VMEM((ROWS, 128, 512), f32),
        pltpu.VMEM((TP, TOK, 128), bf),
        pltpu.SemaphoreType.REGULAR,
        dma((5,)),
        dma((4,)),
    ]
    one = dma
    scratch += [one] * 6
    scratch += [dma((2,)), dma((2,)), one, dma((4,)), one, one, dma((4,))]
    scratch += [one, one, one, dma((4,))]
    scratch += [one, dma((6,)), dma((2,)), one, one]
    return pl.pallas_call(
        kernel,
        out_shape=jax.ShapeDtypeStruct((TOK, D), bf),
        in_specs=[hbm] * 15,
        out_specs=vm,
        scratch_shapes=scratch,
        compiler_params=pltpu.CompilerParams(
            collective_id=0, has_side_effects=True, vmem_limit_bytes=40 * 1024 * 1024
        ),
        name="fused",
    )(
        *(
            pltpu.with_memory_space_constraint(a, pltpu.HBM)
            for a in (
                latent, context, cond.reshape(1, 16), cctx.reshape(1, 16), shw, scw, gw, gain.reshape(1, D),
                wq, wk, wv, qg.reshape(1, HD), kg.reshape(1, HD), bias.transpose(1, 0, 2), outw,
            )
        )
    )


def solution(mesh):
    placed = (
        P("sp", None), P("sp", None), P("sp"), P("sp"),
        P("sp", "tp"), P("sp", "tp"), P("sp", "tp"), P(),
        P(None, "tp"), P(None, "tp"), P(None, "tp"), P(), P(),
        P("tp", None, None), P("tp", None),
    )
    return jax.shard_map(
        per_device, mesh=mesh, in_specs=placed, out_specs=P("sp", None), check_vma=False
    )
```

```python
import jax
import jax.numpy as jnp
from jax import lax
from jax.experimental import pallas as pl
from jax.experimental.pallas import tpu as pltpu
from jax.sharding import PartitionSpec as P

MESH = pl.DeviceIdType.MESH
EPS = 1e-06
Z, Y, TP = 16, 8, 8
SP = Z * Y
D = 2048
F = D // TP
TOK = 256
COLS = 64
ROWS = 4
HD = 64
HALF = D // 2
NEG = float("-inf")


def rem(a, n):
    return lax.rem(a, jnp.int32(n))


def head_norm(p, gain2):
    lane = lax.broadcasted_iota(jnp.int32, p.shape, 1)
    left = lane < HD
    sq = p * p
    s0 = jnp.sum(jnp.where(left, sq, 0.0), axis=1, keepdims=True)
    s1 = jnp.sum(jnp.where(left, 0.0, sq), axis=1, keepdims=True)
    r0 = lax.rsqrt(s0 * (1.0 / HD) + EPS)
    r1 = lax.rsqrt(s1 * (1.0 / HD) + EPS)
    return p * jnp.where(left, r0, r1) * gain2


def kernel(
    latent, context, cond_h, cctx_h, shw_h, scw_h, gw_h, gain_h, wq, wk, wv, qg_h, kg_h, bias_h, outw,
    out,
    cc, modw, gain, qkg, bias,
    part, mody, zpart, modz, modf,
    cbuf, cf, ckv,
    xn, hid, chid,
    wall, wfull, latv,
    tbl, kvp, q2, ew, attb,
    relay, small_sem, loc_sem,
    ys, yr, zs, zr, ts, tr,
    czs, czr, cts, ctr, cpr, cys, cyr,
    hs, hr, ws, wr,
    as_, ar, apr, os_, or_,
):
    sp = lax.axis_index("sp")
    tp = lax.axis_index("tp")
    y = rem(sp, Y)
    z = lax.div(sp, jnp.int32(Y))
    c = rem(tp, 2)
    odd = rem(y + 1, 2)
    mate = rem(y + Y + 1 - 2 * odd, Y)
    side = 2 * odd - 1
    pair = rem(lax.div(y + 1, jnp.int32(2)), 4)
    partner = tp + 1 - 2 * c
    up = rem(sp + 1, SP)
    down = rem(sp + SP - 1, SP)
    right = rem(tp + 2, TP)
    left = rem(tp + TP - 2, TP)
    far = rem(tp + 4, TP)

    def at(s, t):
        return {"sp": s, "tp": t}

    def y_peer(k):
        return at(z * Y + rem(y + k, Y), tp)

    def z_peer(k):
        return at(rem(z + k, Z) * Y + y, tp)

    def m_peer(k):
        return at(rem(z + k, Z) * Y + mate, tp)

    def t_peer(k):
        return at(sp, rem(tp + k, TP))

    def remote(src, dst, s, r, dev):
        return pltpu.make_async_remote_copy(
            src_ref=src, dst_ref=dst, send_sem=s, recv_sem=r, device_id=dev, device_id_type=MESH
        )

    def send(src, dst, s, r, dev):
        remote(src, dst, s, r, dev).start()

    def arrived(ref, r):
        remote(ref, ref, r, r, at(sp, partner)).wait_recv()

    def sent(ref, s):
        remote(ref, ref, s, s, at(sp, partner)).wait_send()

    barrier = pltpu.get_barrier_semaphore()
    near = (4, 12, 3, 13, 2, 14, 1, 15)
    beyond = (8, 7, 9, 6, 10, 5, 11)
    y_order = (4, 3, 5, 2, 6, 1, 7)
    peers = [y_peer(k) for k in y_order]
    peers += [z_peer(k) for k in near] + [m_peer(k) for k in near + (0,)]
    peers += [t_peer(k) for k in range(1, TP)]
    peers += [at(up, tp), at(down, tp)]
    for p in peers:
        pl.semaphore_signal(barrier, inc=1, device_id=p, device_id_type=MESH)

    small = (
        (cond_h, cc.at[0], 0), (cctx_h, cc.at[1], 0),
        (shw_h, modw.at[0], 1), (scw_h, modw.at[1], 1), (gw_h, modw.at[2], 1),
        (bias_h, bias, 2), (gain_h, gain, 3), (qg_h, qkg.at[0], 4), (kg_h, qkg.at[1], 4),
    )
    for src, dst, n in small:
        pltpu.make_async_copy(src, dst, small_sem.at[n]).start()
    ctx_col = pl.multiple_of(tp * F, F)
    my_half = pl.ds(pl.multiple_of(c * HALF, HALF), HALF)
    its_half = pl.ds(pl.multiple_of((1 - c) * HALF, HALF), HALF)
    own_ctx = cbuf.at[tp, odd, z]
    own_c = pltpu.make_async_copy(context.at[:, pl.ds(ctx_col, F)], own_ctx, loc_sem.at[0])
    own_l = pltpu.make_async_copy(latent, latv, loc_sem.at[1])
    own_w = pltpu.make_async_copy(outw.at[:, my_half], wfull.at[tp], loc_sem.at[2])
    own_c.start()
    own_l.start()
    own_w.start()
    for n, src in enumerate((wk, wv, wq)):
        pltpu.make_async_copy(src, wall.at[:, pl.ds(n * 128, 128)], loc_sem.at[3]).start()

    pl.semaphore_wait(barrier, len(peers))
    for k in (4, Z - 4):
        pl.semaphore_signal(relay, inc=1, device_id=z_peer(k), device_id_type=MESH)

    pltpu.make_async_copy(cc, cc, small_sem.at[0]).wait()
    pltpu.make_async_copy(modw, modw, small_sem.at[1]).wait()
    row8 = lax.broadcasted_iota(jnp.int32, (8, 16), 0)
    pre = jnp.where(row8 == 0, jnp.broadcast_to(cc[0], (8, 16)), jnp.broadcast_to(cc[1], (8, 16)))
    act = (pre / (1.0 + jnp.exp(-pre))).astype(jnp.bfloat16)
    p_sh = jnp.dot(act, modw[0], preferred_element_type=jnp.float32)
    p_sc = jnp.dot(act, modw[1], preferred_element_type=jnp.float32)
    p_g = jnp.dot(act, modw[2], preferred_element_type=jnp.float32)
    part[0:2, :] = p_sh[0:2]
    part[2:4, :] = p_sc[0:2]
    part[4:5, :] = p_g[0:1]

    def other(t):
        return t + 1 - 2 * c

    for k in y_order:
        send(part, mody.at[k - 1], ys, yr, y_peer(k))
    own_c.wait()
    for k in near:
        send(own_ctx, own_ctx, czs.at[0], czr.at[0], z_peer(k))
        send(own_ctx, own_ctx, czs.at[1], czr.at[1], m_peer(k))
    send(own_ctx, own_ctx, czs.at[1], czr.at[1], m_peer(0))
    send(outw.at[:, its_half], wfull.at[tp], ws, wr.at[0], at(sp, partner))
    send(outw.at[:, my_half], wfull.at[tp], ws, wr.at[1], at(sp, right))
    send(outw.at[:, my_half], wfull.at[tp], ws, wr.at[1], at(sp, left))
    send(outw.at[:, its_half], wfull.at[tp], ws, wr.at[2], at(sp, other(right)))
    send(outw.at[:, its_half], wfull.at[tp], ws, wr.at[2], at(sp, other(left)))

    pl.semaphore_wait(relay, 2)
    for k in beyond:
        send(own_ctx, own_ctx, czs.at[0], czr.at[0], z_peer(k))
        send(own_ctx, own_ctx, czs.at[1], czr.at[1], m_peer(k))

    arrived(mody, yr)
    acc = part[...]
    for k in range(1, Y):
        acc = acc + mody[k - 1]
    zpart[...] = acc
    for k in beyond + near:
        send(zpart, modz.at[k - 1], zs, zr, z_peer(k))

    tq = lax.broadcasted_iota(jnp.int32, (COLS, 128), 0)
    tl = lax.broadcasted_iota(jnp.int32, (COLS, 128), 1)
    tk = jnp.where(tl < COLS, tl, tl - COLS)
    diff = tk - tq + 15
    c0 = jnp.clip(tq - 8, 0, 48)
    is_open = (tk >= c0) & (tk < c0 + 16)
    first = lax.broadcasted_iota(jnp.int32, (1, 128), 1) < COLS

    def table_step(n, carry):
        h = lax.div(n, jnp.int32(14))
        a = rem(n, 14)
        val = jnp.full((COLS, 128), NEG, jnp.float32)
        for dd in range(31):
            v = jnp.where(first, bias[a, h, dd], bias[a + 1, h, dd])
            val = jnp.where(diff == dd, jnp.broadcast_to(v, (COLS, 128)), val)
        tbl[h, a] = jnp.where(is_open, val, NEG)
        return carry

    pltpu.make_async_copy(bias_h, bias, small_sem.at[2]).wait()
    lax.fori_loop(0, 28, table_step, 0)
    pltpu.make_async_copy(gain_h, gain, small_sem.at[3]).wait()

    def normed(load, store, rows, chunk):
        def step(n, carry):
            r = pl.ds(pl.multiple_of(n * chunk, chunk), chunk)
            v = load(r).astype(jnp.float32)
            ms = jnp.mean(v * v, axis=-1, keepdims=True)
            store(r, v * lax.rsqrt(ms + EPS) * gain[...])
            return carry

        lax.fori_loop(0, rows // chunk, step, 0)

    own_l.wait()

    def store_own(r, v):
        xn[r, :] = v

    normed(lambda r: latv[r, :], store_own, TOK, 16)

    arrived(cbuf.at[0, 0, pl.ds(0, Z - 1)], czr.at[0])
    arrived(cbuf.at[0, 0], czr.at[1])
    hops = ((far, 0), (right, 1), (left, 2), (partner, 3))
    for t, n in hops:
        send(cbuf.at[tp], cbuf.at[tp], cts, ctr.at[n], at(sp, t))

    arrived(modz, zr)
    acc = zpart[...]
    for k in range(1, Z):
        acc = acc + modz[k - 1]
    modf[tp] = acc
    for k in (4, 3, 5, 2, 6, 1, 7):
        send(modf.at[tp], modf.at[tp], ts, tr, t_peer(k))

    def unpack(g):
        cols = pl.ds(pl.multiple_of(g * F, F), F)
        for j in range(2 * Z):
            cf[4 * j : 4 * j + 4, cols] = cbuf[g, j % 2, j // 2].astype(jnp.float32)

    unpack(tp)
    for n, frm in ((1, left), (2, right), (0, far)):
        arrived(cbuf.at[frm], ctr.at[n])
        send(cbuf.at[frm], cbuf.at[frm], cts, cpr, at(sp, partner))
        if n:
            unpack(frm)
    unpack(far)
    arrived(cbuf.at[partner], ctr.at[3])
    unpack(partner)
    arrived(cbuf.at[pl.ds(0, 3)], cpr)
    for frm in (left, right, far):
        unpack(other(frm))

    def store_ctx(r, v):
        cf[r, :] = v

    normed(lambda r: cf[r, :], store_ctx, 128, 16)

    pltpu.make_async_copy(wall, wall, loc_sem.at[3]).wait()
    pltpu.make_async_copy(qkg, qkg, small_sem.at[4]).wait()
    arrived(modf.at[pl.ds(0, TP - 1)], tr)
    lane = lax.broadcasted_iota(jnp.int32, (1, 128), 1)
    qg2 = jnp.concatenate([qkg[0], qkg[0]], axis=1)
    kg2 = jnp.concatenate([qkg[1], qkg[1]], axis=1)

    for g in range(TP):
        gs = slice(g * F, (g + 1) * F)
        chid[:, gs] = (cf[:, gs] * (1.0 + modf[g, 3:4, :]) + modf[g, 1:2, :]).astype(jnp.bfloat16)
    kv = jnp.dot(chid[...], wall[:, 0:256], preferred_element_type=jnp.float32)
    ckv[pair, :, 0:128] = head_norm(kv[:, 0:128], kg2).astype(jnp.bfloat16)
    ckv[pair, :, 128:256] = kv[:, 128:256].astype(jnp.bfloat16)
    zh = rem(z, 2)
    zmate = at((z + 1 - 2 * zh) * Y + y, tp)
    tok_half = pl.ds(pl.multiple_of(zh * 64, 64), 64)
    own_pair = ckv.at[pair, tok_half]
    for k in (3, 2, 1):
        send(own_pair, own_pair, cys, cyr.at[k - 1], at(z * Y + rem(y + k * side + Y, Y), tp))

    for n in range(2):
        r = pl.ds(n * 128, 128)
        for g in range(TP):
            gs = slice(g * F, (g + 1) * F)
            hid[r, gs] = (xn[r, gs] * (1.0 + modf[g, 2:3, :]) + modf[g, 0:1, :]).astype(jnp.bfloat16)
        h = hid[r, :]
        kv = jnp.dot(h, wall[:, 0:256], preferred_element_type=jnp.float32)
        kr = pl.ds(TOK + n * 128, 128)
        kvp[kr, 0:128] = head_norm(kv[:, 0:128], kg2).astype(jnp.bfloat16)
        kvp[kr, 128:256] = kv[:, 128:256].astype(jnp.bfloat16)
    own_rows = kvp.at[pl.ds(TOK, TOK)]
    send(own_rows, kvp.at[pl.ds(0, TOK)], hs, hr, at(up, tp))
    send(own_rows, kvp.at[pl.ds(2 * TOK, TOK)], hs, hr, at(down, tp))

    for n in range(2):
        r = pl.ds(n * 128, 128)
        q = jnp.dot(hid[r, :], wall[:, 256:384], preferred_element_type=jnp.float32)
        q = (head_norm(q, qg2) * (HD**-0.5)).astype(jnp.bfloat16)
        zero = jnp.zeros_like(q)
        lf = jnp.broadcast_to(lane < HD, q.shape)
        q0 = jnp.where(lf, q, zero)
        q1 = jnp.where(lf, zero, q)
        for i in range(2):
            q2[2 * n + i, 0:64, :] = q0[i * 64 : (i + 1) * 64]
            q2[2 * n + i, 64:128, :] = q1[i * 64 : (i + 1) * 64]

    lo, hi = pl.ds(0, 64), pl.ds(64, 64)
    arrived(wfull.at[pl.ds(0, 2)], wr.at[1])
    arrived(wfull.at[pl.ds(0, 2)], wr.at[2])
    for f in (left, other(left)):
        send(wfull.at[f, lo], wfull.at[f, lo], ws, wr.at[3], at(sp, right))
    for f in (right, other(right)):
        send(wfull.at[f, hi], wfull.at[f, hi], ws, wr.at[3], at(sp, left))

    for k, p in ((1, pair + side), (2, pair - side), (3, pair + 2)):
        got = ckv.at[rem(p + 4, 4), tok_half]
        arrived(got, cyr.at[k - 1])
        send(got, got, cys, cyr.at[3], zmate)

    arrived(kvp.at[pl.ds(0, 2 * TOK)], hr)

    nt = (((1,), (1,)), ((), ()))
    at_first = sp == 0
    at_last = sp == SP - 1
    m_w, l_w, band = [], [], []
    for i in range(ROWS):
        start = jnp.where(at_first, 4, jnp.where(at_last, 0, i))
        off = jnp.where(at_first, 7 - i, 3 + jnp.where(at_last, -i, 0))
        rows = pl.ds(pl.multiple_of(start * COLS, COLS), 8 * COLS)
        band.append(rows)
        s = lax.dot_general(q2[i], kvp[rows, 0:128], nt, preferred_element_type=jnp.float32)
        tiles = []
        for p in range(4):
            t = jnp.concatenate([tbl[0, off + 2 * p], tbl[1, off + 2 * p]], axis=0)
            tiles.append(s[:, p * 128 : (p + 1) * 128] + t)
        s = jnp.concatenate(tiles, axis=1)
        m = jnp.max(s, axis=1, keepdims=True)
        e = jnp.exp(s - m)
        ew[i] = e
        m_w.append(m)
        l_w.append(jnp.sum(e, axis=1, keepdims=True))

    arrived(ckv.at[pl.ds(0, 3), pl.ds(0, 64)], cyr.at[3])

    ck = ckv[:, :, 0:128].reshape(512, 128)
    cv = ckv[:, :, 128:256].reshape(512, 128)
    for hh in range(2):
        two = range(2 * hh, 2 * hh + 2)
        s = lax.dot_general(
            q2[2 * hh : 2 * hh + 2].reshape(256, 128), ck, nt, preferred_element_type=jnp.float32
        )
        mw = jnp.concatenate([m_w[i] for i in two], axis=0)
        lw = jnp.concatenate([l_w[i] for i in two], axis=0)
        m = jnp.maximum(mw, jnp.max(s, axis=1, keepdims=True))
        e = jnp.exp(s - m)
        fw = jnp.exp(mw - m)
        inv = 1.0 / (lw * fw + jnp.sum(e, axis=1, keepdims=True))
        o_ctx = jnp.dot((e * inv).astype(jnp.bfloat16), cv, preferred_element_type=jnp.float32)
        fi = fw * inv
        for j, i in enumerate(two):
            w_win = (ew[i] * fi[j * 128 : (j + 1) * 128]).astype(jnp.bfloat16)
            o = jnp.dot(w_win, kvp[band[i], 128:256], preferred_element_type=jnp.float32)
            o = o + o_ctx[j * 128 : (j + 1) * 128]
            o = jnp.where(jnp.broadcast_to(lane < HD, (64, 128)), o[0:64], o[64:128])
            attb[tp, i * COLS : (i + 1) * COLS, :] = o.astype(jnp.bfloat16)
        block = attb.at[tp, pl.ds(hh * 128, 128)]
        for t, n in hops:
            send(block, block, as_, apr.at[hh] if n == 3 else ar.at[hh * 3 + n], at(sp, t))

    for hh in range(2):
        rr = pl.ds(hh * 128, 128)
        for n, frm in ((1, left), (2, right), (0, far)):
            block = attb.at[frm, rr]
            arrived(block, ar.at[hh * 3 + n])
            send(block, block, as_, apr.at[hh], at(sp, partner))

    arrived(wfull.at[partner], wr.at[0])
    own_w.wait()
    arrived(wfull.at[pl.ds(0, 2)], wr.at[3])

    for hh in range(2):
        rr = pl.ds(hh * 128, 128)
        arrived(attb.at[pl.ds(0, 2)], apr.at[hh])
        for n in range(HALF // F):
            cols = pl.ds(pl.multiple_of(c * HALF + n * F, F), F)
            acc = jnp.zeros((128, F), jnp.float32)
            for g in range(TP):
                t = jnp.dot(attb[g, rr, :], wfull[g, :, n * F : (n + 1) * F], preferred_element_type=jnp.float32)
                acc = acc + t.astype(jnp.bfloat16).astype(jnp.float32)
            res = latv[rr, cols].astype(jnp.float32) + modf[c * (HALF // F) + n, 4:5, :] * acc
            out[rr, cols] = res.astype(jnp.bfloat16)
            send(out.at[rr, cols], out.at[rr, cols], os_, or_, at(sp, partner))
    arrived(out.at[:, its_half], or_)

    sent(mody, ys)
    sent(modz, zs)
    sent(modf.at[pl.ds(0, TP - 1)], ts)
    sent(cbuf.at[0, 0, pl.ds(0, Z - 1)], czs.at[0])
    sent(cbuf.at[0, 0], czs.at[1])
    sent(cbuf.at[pl.ds(0, 7)], cts)
    sent(ckv.at[pl.ds(0, 3)], cys)
    sent(kvp.at[pl.ds(0, 2 * TOK)], hs)
    sent(wfull.at[pl.ds(0, 7)], ws)
    sent(attb.at[pl.ds(0, 7)], as_)
    sent(out.at[:, my_half], os_)


def per_device(latent, context, cond, cctx, shw, scw, gw, gain, wq, wk, wv, qg, kg, bias, outw):
    hbm = pl.BlockSpec(memory_space=pltpu.HBM)
    vm = pl.BlockSpec(memory_space=pltpu.VMEM)
    bf, f32 = jnp.bfloat16, jnp.float32
    dma = pltpu.SemaphoreType.DMA
    scratch = [
        pltpu.VMEM((2, 1, 16), f32),
        pltpu.VMEM((3, 16, F), bf),
        pltpu.VMEM((1, D), f32),
        pltpu.VMEM((2, 1, HD), f32),
        pltpu.SMEM((15, 2, 31), f32),
        pltpu.VMEM((5, F), f32),
        pltpu.VMEM((Y - 1, 5, F), f32),
        pltpu.VMEM((5, F), f32),
        pltpu.VMEM((Z - 1, 5, F), f32),
        pltpu.VMEM((TP, 5, F), f32),
        pltpu.VMEM((TP, 2, Z, 4, F), bf),
        pltpu.VMEM((128, D), f32),
        pltpu.VMEM((4, 128, 256), bf),
        pltpu.VMEM((TOK, D), f32),
        pltpu.VMEM((TOK, D), bf),
        pltpu.VMEM((128, D), bf),
        pltpu.VMEM((D, 384), bf),
        pltpu.VMEM((TP, 128, HALF), bf),
        pltpu.VMEM((TOK, D), bf),
        pltpu.VMEM((2, 14, COLS, 128), f32),
        pltpu.VMEM((3 * TOK, 256), bf),
        pltpu.VMEM((ROWS, 128, 128), bf),
        pltpu.VMEM((ROWS, 128, 512), f32),
        pltpu.VMEM((TP, TOK, 128), bf),
        pltpu.SemaphoreType.REGULAR,
        dma((5,)),
        dma((4,)),
    ]
    one = dma
    scratch += [one] * 6
    scratch += [dma((2,)), dma((2,)), one, dma((4,)), one, one, dma((4,))]
    scratch += [one, one, one, dma((4,))]
    scratch += [one, dma((6,)), dma((2,)), one, one]
    return pl.pallas_call(
        kernel,
        out_shape=jax.ShapeDtypeStruct((TOK, D), bf),
        in_specs=[hbm] * 15,
        out_specs=vm,
        scratch_shapes=scratch,
        compiler_params=pltpu.CompilerParams(
            collective_id=0, has_side_effects=True, vmem_limit_bytes=40 * 1024 * 1024
        ),
        name="fused",
    )(
        *(
            pltpu.with_memory_space_constraint(a, pltpu.HBM)
            for a in (
                latent, context, cond.reshape(1, 16), cctx.reshape(1, 16), shw, scw, gw, gain.reshape(1, D),
                wq, wk, wv, qg.reshape(1, HD), kg.reshape(1, HD), bias.transpose(1, 0, 2), outw,
            )
        )
    )


def solution(mesh):
    placed = (
        P("sp", None), P("sp", None), P("sp"), P("sp"),
        P("sp", "tp"), P("sp", "tp"), P("sp", "tp"), P(),
        P(None, "tp"), P(None, "tp"), P(None, "tp"), P(), P(),
        P("tp", None, None), P("tp", None),
    )
    return jax.shard_map(
        per_device, mesh=mesh, in_specs=placed, out_specs=P("sp", None), check_vma=False
    )
```
